256 devices in a mesh: sp: 16 (over y, x), tp: 16 (over z, core).
Axes of the slice: x: 4, y: 4, z: 8, core: 2. Of those that a mesh axis runs over, the one named last changes fastest.
Arguments:
- residual_in: bfloat16 [4096, 4096], P(('sp', 'tp')), may hold values from -6 to 6
- queries: bfloat16 [4096, 2048], P('sp', 'tp'), may hold values from -6 to 6
- keys: bfloat16 [4096, 2048], P('sp', 'tp'), may hold values from -6 to 6
- values: bfloat16 [4096, 2048], P('sp', 'tp'), may hold values from -6 to 6
- break_offset: bfloat16 [4096, 32], P('sp', 'tp'), may hold values from -14 to 1
- doc_ids: int32 [4096], P('sp'), may hold values from 0 to 2, never falling along the last dimension, each value on 1 to 2560 neighbouring positions
- out_weight: bfloat16 [2048, 4096], P('tp'), may hold values from -0.125 to 0.125
- norm_gain: float32 [4096], replicated, may hold values from 0.1 to 1.9
- group_router: bfloat16 [4096, 2], replicated, may hold values from -0.1875 to 0.1875
- expert_router: bfloat16 [4096, 16], replicated, may hold values from -0.1875 to 0.1875
- expert_ids: int32 [4096, 2], P('sp'), may hold values from 0 to 15, as said below
- gate_weight: bfloat16 [16, 4096, 4096], P('sp', None, 'tp'), may hold values from -0.09375 to 0.09375
- up_weight: bfloat16 [16, 4096, 4096], P('sp', None, 'tp'), may hold values from -0.09375 to 0.09375
- down_weight: bfloat16 [16, 4096, 4096], P('sp', 'tp'), may hold values from -0.09375 to 0.09375
Outputs:
- layer_out: bfloat16 [4096, 4096], P(('sp', 'tp'))
The draws below stay inside these ranges and needn't reach their ends.
Inputs may be any that keep to these rules, and one draw needn't show every extreme that they name: `doc_ids`: document numbers never fall along the positions; one document covers exactly 2560 positions. `expert_ids`: the two experts of a position differ and lie in one group of 8 consecutive numbers; in each aligned block of 16 positions every expert is named exactly 2 times.
All inputs are finite; a program needn't handle non-finite values.
Results may differ from the reference program's by a relative error of at most 0.013.
Values may be sent and summed in bfloat16 or wider, within the bound.
A program may use at most 64 MiB of HBM per device.

```python
import math
import jax
import jax.numpy as jnp
import numpy as np
from jax import lax

D = 4096
ATTENTION_HEADS = 32
HEAD_DIM = 64
ATT = 2048
D_EXPERT = 4096
GROUPS = 2
EXPERTS = 16
GROUP_EXPERTS = 8
TOK_DEV = 256
SEQUENCE_TOKENS = 4096
ROWS_DEV = 16
KEY_BLOCK = 256
DOCS = 3
DOC_MOST = 2560
N_TP = 16


def draw_break_offset(key, part):
    gathered_keys = jax.random.split(jax.random.fold_in(key, 7), 5)
    lagging_heads = jax.random.uniform(gathered_keys[0], (ATTENTION_HEADS,)) < 0.5
    factor = jnp.exp(jax.random.uniform(gathered_keys[1], (SEQUENCE_TOKENS // TOK_DEV, 1), minval=0.0, maxval=math.log(4.0)))
    factor = jnp.repeat(factor, TOK_DEV, axis=0)
    slow_level = jnp.log(0.1 * factor / SEQUENCE_TOKENS)
    fast_level = jnp.log(factor / 48.0)
    jitter = 0.5 * jax.random.normal(gathered_keys[2], (SEQUENCE_TOKENS, ATTENTION_HEADS))
    logging_level = jnp.where(lagging_heads[None, :], slow_level, fast_level) + jitter
    spike_matched = jax.random.uniform(gathered_keys[3], (SEQUENCE_TOKENS, ATTENTION_HEADS)) < 6.0 / SEQUENCE_TOKENS
    spike_value = jax.random.uniform(gathered_keys[4], (SEQUENCE_TOKENS, ATTENTION_HEADS), minval=-1.0, maxval=0.0)
    document_starts = jnp.where(spike_matched & lagging_heads[None, :], spike_value, logging_level)
    return jnp.clip(document_starts, -14.0, 1.0).astype(jnp.bfloat16)


def draw_expert_ids(key, part):
    routing_key = jax.random.fold_in(key, 13)
    blocks = SEQUENCE_TOKENS // ROWS_DEV
    per_group = ROWS_DEV // GROUPS
    group_size = EXPERTS // GROUPS
    block_keys = jax.random.split(routing_key, blocks)

    def one_block(block_key):
        perm_key, relabel_key, swap_key = jax.random.split(block_key, 3)
        row_rank = jax.random.permutation(perm_key, ROWS_DEV)
        group_index = row_rank // per_group
        inner_rank = row_rank % per_group
        relabel = jax.vmap(lambda sub_key: jax.random.permutation(sub_key, group_size))(jax.random.split(relabel_key, GROUPS))
        first = relabel[group_index, inner_rank % group_size]
        second = relabel[group_index, (inner_rank + 1) % group_size]
        swapped = jax.random.randint(swap_key, (ROWS_DEV,), 0, 2)
        lower_id = jnp.where(swapped == 1, second, first)
        upper_id = jnp.where(swapped == 1, first, second)
        return jnp.stack([group_index * group_size + lower_id, group_index * group_size + upper_id], axis=1)
    return jax.vmap(one_block)(block_keys).reshape(SEQUENCE_TOKENS, 2).astype(jnp.int32)


def block_levels(key, shape, shards, smallest, largest):
    loudness, own = 1.0, jax.random.fold_in(key, 6)
    for axis_at, blocks in shards:
        draws = jnp.exp(jax.random.uniform(jax.random.fold_in(own, axis_at), (blocks,), jnp.float32, smallest / len(shards), largest / len(shards)))
        loudness = loudness * jnp.repeat(draws, shape[axis_at] // blocks).reshape([-1 if axis == axis_at else 1 for axis in range(len(shape))])
    return loudness


def profile(amount, total, bound, skew):
    portions = [(1 << 20) // math.isqrt(grade ** skew) + 1 for grade in range(2, amount + 1)]
    surplus, holding = total - bound - (amount - 1), [1] * (amount - 1)
    while surplus > 0:
        movable = [i for i in range(amount - 1) if holding[i] < bound]
        mass, left = sum([portions[i] for i in movable]), surplus
        for i in movable:
            extra = min(bound - holding[i], max(1, left * portions[i] // mass), surplus)
            holding[i] = holding[i] + extra
            surplus = surplus - extra
    return np.array([bound] + holding)


def ragged(rng, amount, total, bound, lean):
    if amount == 2:
        one = jax.random.randint(rng, (), max(1, total - bound), min(bound, total - 1) + 1)
        return jnp.stack([one, total - one])
    lengths = jnp.asarray(profile(amount, total, bound, lean), jnp.int32)
    twos = (amount - 1) // 2
    donor, sink = lengths[1:1 + 2 * twos:2], lengths[2:2 + 2 * twos:2]
    room = jnp.minimum(donor - 1, bound - sink)
    passed = jax.random.randint(jax.random.fold_in(rng, 1), (twos,), 0, 1 << 20) % (room + 1)
    lengths = lengths.at[1:1 + 2 * twos:2].set(donor - passed).at[2:2 + 2 * twos:2].set(sink + passed)
    return lengths[jax.random.permutation(jax.random.fold_in(rng, 2), amount)]


def gaussian(stream_key, dims, width, bound, cuts=(), held_as=jnp.bfloat16):
    result = jax.random.normal(stream_key, dims, jnp.float32) * width
    if len(cuts) > 0:
        result = block_levels(stream_key, dims, cuts, -0.22, 0.18) * result
    return jnp.clip(result, min=-bound, max=bound).astype(held_as)


def setup_inputs(seed: int = 0) -> dict:
    seeds = jax.random.split(jax.random.key(seed), 15)
    return {
        "residual_in": gaussian(seeds[0], (SEQUENCE_TOKENS, D), 1.0, 6.0, ((0, 256),)),
        "queries": gaussian(seeds[1], (SEQUENCE_TOKENS, ATT), 1.0, 6.0, ((0, 16), (1, 16))),
        "keys": gaussian(seeds[2], (SEQUENCE_TOKENS, ATT), 1.0, 6.0, ((0, 16), (1, 16))),
        "values": gaussian(seeds[3], (SEQUENCE_TOKENS, ATT), 1.0, 6.0, ((0, 16), (1, 16))),
        "break_offset": draw_break_offset(jax.random.fold_in(seeds[14], 71), 0),
        "doc_ids": jnp.searchsorted(jnp.cumsum(ragged(seeds[5], DOCS, SEQUENCE_TOKENS, DOC_MOST, 0)), jnp.arange(SEQUENCE_TOKENS), side="right").astype(jnp.int32),
        "out_weight": gaussian(seeds[6], (ATT, D), ATT ** -0.5, 0.125, ((0, 16),)),
        "norm_gain": jnp.clip(1.0 + 0.18 * jax.random.normal(seeds[7], (D,), jnp.float32), 0.1, 1.9),
        "group_router": gaussian(seeds[8], (D, GROUPS), (D // 4) ** -0.5, 0.1875),
        "expert_router": gaussian(seeds[9], (D, EXPERTS), (D // 4) ** -0.5, 0.1875),
        "expert_ids": draw_expert_ids(jax.random.fold_in(seeds[14], 71), 0),
        "gate_weight": gaussian(seeds[11], (EXPERTS, D, D_EXPERT), D ** -0.5, 0.09375, ((0, 16), (2, 16))),
        "up_weight": gaussian(seeds[12], (EXPERTS, D, D_EXPERT), D ** -0.5, 0.09375, ((0, 16), (2, 16))),
        "down_weight": gaussian(seeds[13], (EXPERTS, D_EXPERT, D), D_EXPERT ** -0.5, 0.09375, ((0, 16), (1, 16))),
    }


def block_result(query_head, key_block, value_block, offset_block, query_pos, query_doc, key_pos, key_doc):
    scores = jnp.dot(query_head, key_block.T, preferred_element_type=jnp.float32) * HEAD_DIM ** (-0.5)
    scores = scores + offset_block.astype(jnp.float32)[None, :]
    live_mask = (key_pos[None, :] < query_pos[:, None]) & (key_doc[None, :] == query_doc[:, None])
    stay_log = jnp.where(live_mask, jax.nn.log_sigmoid(-scores), jnp.float32(0.0))
    within = lax.cumsum(stay_log, axis=1, reverse=True) - stay_log
    weights = jnp.where(live_mask, jnp.exp(jax.nn.log_sigmoid(scores) + within), jnp.float32(0.0)).astype(jnp.bfloat16)
    partial_out = jnp.dot(weights, value_block, preferred_element_type=jnp.float32)
    return (partial_out, lax.optimization_barrier(jnp.sum(stay_log, axis=1)))

def attend(queries, keys, values, break_offset, doc_ids):
    positions = jnp.arange(SEQUENCE_TOKENS, dtype=jnp.int32)
    query_heads = queries.reshape(SEQUENCE_TOKENS, ATTENTION_HEADS, HEAD_DIM).transpose(1, 0, 2)
    key_heads = keys.reshape(SEQUENCE_TOKENS, ATTENTION_HEADS, HEAD_DIM).transpose(1, 0, 2)
    value_heads = values.reshape(SEQUENCE_TOKENS, ATTENTION_HEADS, HEAD_DIM).transpose(1, 0, 2)
    document_starts = break_offset.T
    block_count = SEQUENCE_TOKENS // KEY_BLOCK

    def one_head(operands):
        query_head, key_head, value_head, offset_head = operands

        def advance(running, block_index):
            out_sum, stay_sum = running
            block_begin = (block_index * KEY_BLOCK).astype(jnp.int32)
            key_block = lax.dynamic_slice_in_dim(key_head, block_begin, KEY_BLOCK, 0)
            value_block = lax.dynamic_slice_in_dim(value_head, block_begin, KEY_BLOCK, 0)
            offset_block = lax.dynamic_slice_in_dim(offset_head, block_begin, KEY_BLOCK, 0)
            key_doc = lax.dynamic_slice_in_dim(doc_ids, block_begin, KEY_BLOCK, 0)
            key_pos = block_begin + jnp.arange(KEY_BLOCK, dtype=jnp.int32)
            partial_out, totals = block_result(query_head, key_block, value_block, offset_block, positions, doc_ids, key_pos, key_doc)
            out_sum = out_sum + jnp.exp(stay_sum)[:, None] * partial_out
            return ((out_sum, stay_sum + totals), None)
        initial = (jnp.zeros((SEQUENCE_TOKENS, HEAD_DIM), jnp.float32), jnp.zeros((SEQUENCE_TOKENS,), jnp.float32))
        final, unused = lax.scan(advance, initial, jnp.arange(block_count, dtype=jnp.int32), reverse=True)
        return final[0]
    mixed = lax.map(one_head, (query_heads, key_heads, value_heads, document_starts))
    return mixed.transpose(1, 0, 2).reshape(SEQUENCE_TOKENS, ATTENTION_HEADS * HEAD_DIM).astype(jnp.bfloat16)

def reference(residual_in, queries, keys, values, break_offset, doc_ids, out_weight, norm_gain, group_router, expert_router, expert_ids, gate_weight, up_weight, down_weight):
    attended = attend(queries, keys, values, break_offset, doc_ids)
    width_part = ATTENTION_HEADS * HEAD_DIM // N_TP

    def add_group(running, group_index):
        block_begin = (group_index * width_part).astype(jnp.int32)
        part_in = lax.dynamic_slice_in_dim(attended, block_begin, width_part, 1)
        part_weight = lax.dynamic_slice_in_dim(out_weight, block_begin, width_part, 0)
        product = lax.optimization_barrier(jnp.dot(part_in, part_weight, preferred_element_type=jnp.float32).astype(jnp.bfloat16))
        return (running + product.astype(jnp.float32), None)
    summed, unused = lax.scan(add_group, residual_in.astype(jnp.float32), jnp.arange(N_TP, dtype=jnp.int32))
    mixed_stream = summed.astype(jnp.bfloat16)
    stream_f = mixed_stream.astype(jnp.float32)
    scaling = lax.rsqrt(lax.optimization_barrier(jnp.mean(stream_f * stream_f, axis=1, keepdims=True)) + 1e-06)
    normed = (stream_f * scaling * norm_gain[None, :]).astype(jnp.bfloat16)
    group_logits = jnp.dot(normed, group_router, preferred_element_type=jnp.float32)
    expert_logits = jnp.dot(normed, expert_router, preferred_element_type=jnp.float32)
    chosen_group = expert_ids[:, 0] // GROUP_EXPERTS
    margin = group_logits[:, 0] - group_logits[:, 1]
    own_margin = jnp.where(chosen_group == 0, margin, -margin)
    picked = jnp.take_along_axis(expert_logits, expert_ids, axis=1)
    routes = jax.nn.sigmoid(own_margin)[:, None] * jax.nn.sigmoid(picked - picked[:, ::-1])
    flat_ids = expert_ids.reshape(-1)
    per_expert = 2 * SEQUENCE_TOKENS // EXPERTS
    slice_units = D_EXPERT // N_TP

    def one_expert(operands):
        expert_index, gate_part, up_part, down_part = operands
        row_index = jnp.nonzero(flat_ids == expert_index, size=per_expert)[0].astype(jnp.int32)
        row_block = normed[row_index // 2]
        gate_val = jnp.dot(row_block, gate_part, preferred_element_type=jnp.float32)
        up_val = jnp.dot(row_block, up_part, preferred_element_type=jnp.float32)
        hidden = (jax.nn.silu(gate_val) * up_val).astype(jnp.bfloat16)

        def add_slice(running, slice_index):
            block_begin = (slice_index * slice_units).astype(jnp.int32)
            part_hidden = lax.dynamic_slice_in_dim(hidden, block_begin, slice_units, 1)
            part_down = lax.dynamic_slice_in_dim(down_part, block_begin, slice_units, 0)
            product = lax.optimization_barrier(jnp.dot(part_hidden, part_down, preferred_element_type=jnp.float32).astype(jnp.bfloat16))
            return (running + product.astype(jnp.float32), None)
        initial = jnp.zeros((per_expert, D), jnp.float32)
        total_out, unused_slices = lax.scan(add_slice, initial, jnp.arange(N_TP, dtype=jnp.int32))
        return (total_out.astype(jnp.bfloat16), row_index)
    outputs, indices = lax.map(one_expert, (jnp.arange(EXPERTS, dtype=jnp.int32), gate_weight, up_weight, down_weight))
    expert_out = jnp.zeros((SEQUENCE_TOKENS * 2, D), jnp.bfloat16).at[indices.reshape(-1)].set(outputs.reshape(-1, D))
    expert_out = expert_out.reshape(SEQUENCE_TOKENS, 2, D)
    mixture = lax.optimization_barrier(jnp.sum(routes[:, :, None] * expert_out.astype(jnp.float32), axis=1))
    return (stream_f + mixture).astype(jnp.bfloat16)
```

```python
import functools

import jax
import jax.numpy as jnp
from jax import lax
from jax.experimental import pallas as pl
from jax.experimental.pallas import tpu as pltpu
from jax.sharding import Mesh
from jax.sharding import PartitionSpec as P

HEAD_DIM = 64
GROUPS = 2
DOC_MOST = 2560
KB = 256
MESH = pl.DeviceIdType.MESH
AXES = ("y", "x", "z", "c")
SP = ("y", "x")
TP = ("z", "c")
VM = pl.BlockSpec(memory_space=pltpu.VMEM)
ANY = pl.BlockSpec(memory_space=pl.ANY)
BF = jnp.bfloat16
F32 = jnp.float32
LIMIT = 60 * 1024 * 1024


def dot(a, b):
    return jnp.dot(a, b, preferred_element_type=F32)


def place():
    return tuple(lax.axis_index(a) for a in AXES)


def remote(src, dst, ss, rs, to):
    return pltpu.make_async_remote_copy(
        src_ref=src, dst_ref=dst, send_sem=ss, recv_sem=rs, device_id=to, device_id_type=MESH
    )


def greet(peers):
    bar = pltpu.get_barrier_semaphore()
    for p in peers:
        pl.semaphore_signal(bar, inc=1, device_id=p, device_id_type=MESH)
    pl.semaphore_wait(bar, len(peers))


def gather_kernel(band, ny, nx, k, v, a, w, ko, vo, ao, wo, ks, kr, vs, vr, as_, ar, ws, wr):
    y, x, z, c = place()
    me = y * nx + x
    xs = [lax.rem(x + d, nx) for d in range(1, nx)]
    ys = [lax.rem(y + d, ny) for d in range(1, ny)]
    xb = [lax.rem(x + nx - d, nx) for d in range(1, nx)]
    yb = [lax.rem(y + ny - d, ny) for d in range(1, ny)]
    half = wo.shape[1]
    greet(
        [(y, q, z, c) for q in xs] + [(q, x, z, c) for q in ys] + [(y, x, z, 1 - c)]
    )

    def used(b, j):
        return (j > b) & (j - b <= band)

    def k_first(xs_, xd):
        return (xd > xs_) | (y < ny - 1)

    def v_first(yd, ys_, xs_):
        return (yd > ys_) & (nx * (yd - ys_) - xs_ <= band)

    wcopy = remote(w.at[:, pl.ds((1 - c) * half, half)], wo, ws, wr, (y, x, z, 1 - c))

    def kcopy(b, src, asrc, n, to):
        return (
            remote(src, ko.at[b], ks.at[n], kr.at[b], to),
            remote(asrc, ao.at[b], as_.at[n], ar.at[b], to),
        )

    def vcopy(b, src, n, to):
        return (remote(src, vo.at[b], vs.at[n], vr.at[b], to),)

    plan = []
    wants = []

    def send(cond, copies):
        plan.append((cond, copies))

        @pl.when(cond)
        def _():
            for q in copies:
                q.start()

    def arrive(cond, copies):
        @pl.when(cond)
        def _():
            for q in copies:
                q.wait_recv()

    n = 0
    for q in xs:
        send(k_first(x, q), kcopy(me, k, a, n, (y, q, z, c)))
        n += 1
    m = 0
    for q in ys:
        send(v_first(q, y, x), vcopy(me, v, m, (q, x, z, c)))
        m += 1
    for q in ys:
        send(used(me, q * nx + x), kcopy(me, k, a, n, (q, x, z, c)))
        n += 1
    for q in xs:
        send(used(me, y * nx + q), vcopy(me, v, m, (y, q, z, c)))
        m += 1
    wcopy.start()
    ko[me] = k[...]
    vo[me] = v[...]
    ao[me] = a[...]
    for i in range(max(nx, ny) - 1):
        if i < nx - 1:
            b = y * nx + xb[i]
            got = k_first(xb[i], x)
            arrive(got, kcopy(b, k, a, 0, (y, x, z, c)))
            for q in ys:
                send(got & used(b, q * nx + x), kcopy(b, ko.at[b], ao.at[b], n, (q, x, z, c)))
                n += 1
        if i < ny - 1:
            b = yb[i] * nx + x
            got = v_first(y, yb[i], x)
            arrive(got, vcopy(b, v, 0, (y, x, z, c)))
            for q in xs:
                send(got & used(b, y * nx + q), vcopy(b, vo.at[b], m, (y, q, z, c)))
                m += 1
    for qy in yb:
        for qx in [x] + xb:
            b = qy * nx + qx
            arrive(used(b, me), kcopy(b, k, a, 0, (y, x, z, c)))
    for qx in xb:
        for qy in [y] + yb:
            b = qy * nx + qx
            arrive(used(b, me), vcopy(b, v, 0, (y, x, z, c)))
    for cond, copies in plan:

        @pl.when(cond)
        def _(copies=copies):
            for q in copies:
                q.wait_send()

    wcopy.wait()


def gather_keys(k, v, a, w, ny, nx, cid):
    n = ny * nx
    sends = (nx - 1) + (ny - 1) + (nx - 1) * (ny - 1)
    half = w.shape[1] // 2
    dma = pltpu.SemaphoreType.DMA
    return pl.pallas_call(
        functools.partial(gather_kernel, DOC_MOST // KB, ny, nx),
        out_shape=(
            jax.ShapeDtypeStruct((n,) + k.shape, BF),
            jax.ShapeDtypeStruct((n,) + v.shape, BF),
            jax.ShapeDtypeStruct((n,) + a.shape, BF),
            jax.ShapeDtypeStruct((w.shape[0], half), BF),
        ),
        in_specs=[VM, VM, VM, VM],
        out_specs=(VM, VM, VM, VM),
        scratch_shapes=[
            dma((sends,)), dma((n,)), dma((sends,)), dma((n,)), dma((sends,)), dma((n,)), dma, dma,
        ],
        compiler_params=pltpu.CompilerParams(
            collective_id=cid, has_side_effects=True, vmem_limit_bytes=LIMIT
        ),
        name="gather_keys",
    )(k, v, a, w)


def attend_kernel(band, nx, q, k, v, a, qdoc, o):
    y, x, z, c = place()
    me = y * nx + x
    rows = q.shape[0]
    heads = q.shape[1] // HEAD_DIM
    tri_r = lax.broadcasted_iota(jnp.int32, (KB, KB), 0)
    tri_c = lax.broadcasted_iota(jnp.int32, (KB, KB), 1)
    later = (tri_r > tri_c).astype(BF)
    qh = [q[:, h * HEAD_DIM : (h + 1) * HEAD_DIM] * BF(HEAD_DIM**-0.5) for h in range(heads)]
    qd = qdoc[...]

    def step(t, carry):
        b = me - t
        kb = k[b]
        vb = v[b]
        ab = a[b].astype(F32)
        live = ab[heads : heads + 1, :] == qd
        live = live & ((t > 0) | (tri_c < tri_r))
        new = []
        for h in range(heads):
            out, stay_sum = carry[h]
            kh = kb[:, h * HEAD_DIM : (h + 1) * HEAD_DIM]
            vh = vb[:, h * HEAD_DIM : (h + 1) * HEAD_DIM]
            s = lax.dot_general(
                qh[h], kh, (((1,), (1,)), ((), ())), preferred_element_type=F32
            )
            s = s + ab[h : h + 1, :]
            soft = jnp.log1p(jnp.exp(-jnp.abs(s)))
            stay = jnp.where(live, -(jnp.maximum(s, 0.0) + soft), 0.0)
            hi = stay.astype(BF)
            lo = (stay - hi.astype(F32)).astype(BF)
            within = dot(hi, later) + dot(lo, later)
            wt = jnp.where(live, jnp.exp(jnp.minimum(s, 0.0) - soft + within), 0.0).astype(BF)
            out = out + jnp.exp(stay_sum) * dot(wt, vh)
            stay_sum = stay_sum + jnp.sum(stay, axis=1, keepdims=True)
            new.append((out, stay_sum))
        return tuple(new)

    zero = tuple(
        (jnp.zeros((rows, HEAD_DIM), F32), jnp.zeros((rows, 1), F32)) for _ in range(heads)
    )
    done = lax.fori_loop(0, jnp.minimum(me, band) + 1, step, zero)
    for h in range(heads):
        o[:, h * HEAD_DIM : (h + 1) * HEAD_DIM] = done[h][0].astype(BF)


def attend(q, k, v, a, qdoc, nx):
    return pl.pallas_call(
        functools.partial(attend_kernel, DOC_MOST // KB, nx),
        out_shape=jax.ShapeDtypeStruct(q.shape, BF),
        in_specs=[VM] * 5,
        out_specs=VM,
        compiler_params=pltpu.CompilerParams(vmem_limit_bytes=LIMIT),
        name="attend",
    )(q, k, v, a, qdoc)


def ring_ids(z, nz):
    return lax.rem(z + 1, nz), lax.rem(z + nz - 1, nz)


def project_kernel(nz, nsub, att, w, wsib, res, out, pair, part, sbuf, rbuf, xbuf, ybuf,
                   ds, dr, ss, rs, es, er):
    y, x, z, c = place()
    right, left = ring_ids(z, nz)
    sib = (y, x, z, 1 - c)
    half = w.shape[1] // 2
    kd = att.shape[1]
    greet([(y, x, right, c), (y, x, left, c), sib])
    first = remote(att, pair, ds, dr, sib)
    first.start()
    rows = att.shape[0]
    chunk = rows // nz
    hr = chunk // 2
    part[...] = dot(att[...], w[:, pl.ds(pl.multiple_of(c * half, half), half)])
    first.wait()
    part[...] += dot(pair[...], wsib[...])
    width = half // nsub

    def ring(d, s, j):
        to = right if d == 0 else left
        return remote(
            sbuf.at[d, s, :, pl.ds(j * width, width)],
            rbuf.at[d, s, :, pl.ds(j * width, width)],
            ss.at[d, s, j],
            rs.at[d, s, j],
            (y, x, to, c),
        )

    def own(d, s, j):
        zz = lax.rem(z + nz - 1 - s, nz) if d == 0 else lax.rem(z + 1 + s, nz)
        begin = pl.multiple_of(zz * chunk + d * hr, hr)
        return part[pl.ds(begin, hr), j * width : (j + 1) * width]

    for s in range(nz - 1):
        for j in range(nsub):
            for d in range(2):
                cols = slice(j * width, (j + 1) * width)
                val = own(d, s, j)
                if s > 0:
                    ring(d, s - 1, j).wait_recv()
                    val = val + rbuf[d, s - 1, :, cols].astype(F32)
                sbuf[d, s, :, cols] = val.astype(BF)
                ring(d, s, j).start()
    swap = remote(xbuf, ybuf, es, er, sib)
    mine = []
    for d in range(2):
        tot = []
        for j in range(nsub):
            cols = slice(j * width, (j + 1) * width)
            ring(d, nz - 2, j).wait_recv()
            tot.append(own(d, nz - 1, j) + rbuf[d, nz - 2, :, cols].astype(F32))
        mine.append(jnp.concatenate(tot, axis=1))
    keep = jnp.where(c == 0, mine[0], mine[1])
    xbuf[...] = jnp.where(c == 0, mine[1], mine[0])
    swap.start()
    swap.wait()
    got = ybuf[...]
    low = jnp.where(c == 0, keep, got)
    high = jnp.where(c == 0, got, keep)
    out[:, :half] = (res[:, :half].astype(F32) + low).astype(BF)
    out[:, half:] = (res[:, half:].astype(F32) + high).astype(BF)
    for s in range(nz - 1):
        for j in range(nsub):
            for d in range(2):
                ring(d, s, j).wait_send()


def project(att, w, wsib, res, nz, cid):
    half = w.shape[1] // 2
    hr = att.shape[0] // nz // 2
    nsub = 2
    dma = pltpu.SemaphoreType.DMA
    return pl.pallas_call(
        functools.partial(project_kernel, nz, nsub),
        out_shape=jax.ShapeDtypeStruct(res.shape, BF),
        in_specs=[VM] * 4,
        out_specs=VM,
        scratch_shapes=[
            pltpu.VMEM(att.shape, BF),
            pltpu.VMEM((att.shape[0], half), F32),
            pltpu.VMEM((2, nz - 1, hr, half), BF),
            pltpu.VMEM((2, nz - 1, hr, half), BF),
            pltpu.VMEM((hr, half), F32),
            pltpu.VMEM((hr, half), F32),
            dma, dma,
            dma((2, nz - 1, nsub)), dma((2, nz - 1, nsub)),
            dma, dma,
        ],
        compiler_params=pltpu.CompilerParams(
            collective_id=cid, has_side_effects=True, vmem_limit_bytes=LIMIT
        ),
        name="project",
    )(att, w, wsib, res)


def expert_kernel(ny, nx, nz, nsub, sent, gate, up, down, out,
                  gw, uw, dw, dsib, inb, rows, hid, sbuf, rbuf, fin, lsem,
                  ws, wr, is_, ir, gs, gr, cs, cr, hs, hr_, ss, rs, fs, fr):
    y, x, z, c = place()
    me = y * nx + x
    n = ny * nx
    right, left = ring_ids(z, nz)
    sib = (y, x, z, 1 - c)
    units = dw.shape[0]
    half = dw.shape[1]
    width_all = 2 * half
    per = 2 * n
    loads = [
        pltpu.make_async_copy(gate, gw, lsem.at[0]),
        pltpu.make_async_copy(up, uw, lsem.at[1]),
        pltpu.make_async_copy(
            down.at[:, pl.ds(pl.multiple_of(c * half, half), half)], dw, lsem.at[2]
        ),
    ]
    for q in loads:
        q.start()
    others = []
    for d in range(1, n):
        t = lax.rem(me + d, n)
        others.append((lax.div(t, nx), lax.rem(t, nx), t))
    greet(
        [(ty, tx, z, c) for ty, tx, t in others]
        + [(ty, tx, z, 1 - c) for ty, tx, t in others]
        + [(y, x, right, c), (y, x, left, c), sib]
    )
    wcopy = remote(
        down.at[:, pl.ds(pl.multiple_of((1 - c) * half, half), half)], dsib, ws, wr, sib
    )
    for d, (ty, tx, t) in enumerate(others):
        remote(sent.at[t], inb.at[me], is_.at[d], ir.at[me], (ty, tx, z, c)).start()
    wcopy.start()
    inb[me] = sent[me]
    for ty, tx, t in others:
        remote(sent.at[t], inb.at[t], is_.at[0], ir.at[t], (y, x, z, c)).wait_recv()
    mine = z * 2 + c
    for e in range(n):
        rows[mine, 2 * e : 2 * e + 2, :] = inb[e]

    hb = per // 2

    def piece(b, p):
        return rows.at[b, pl.ds(p * hb, hb), :]

    def hop(d, h, p):
        zz = lax.rem(z + nz - (h - 1), nz) if d == 0 else lax.rem(z + h - 1, nz)
        to = right if d == 0 else left
        b = zz * 2 + c
        return remote(piece(b, p), piece(b, p), gs.at[d, h, p], gr.at[d, h, p], (y, x, to, c))

    def got(d, h, p):
        zz = lax.rem(z + nz - h, nz) if d == 0 else lax.rem(z + h, nz)
        b = zz * 2 + c
        to = right if d == 0 else left
        return b, remote(piece(b, p), piece(b, p), gs.at[d, h, p], gr.at[d, h, p], (y, x, to, c))

    def cross(b, d, h, p):
        return remote(piece(b, p), piece(b, p), cs.at[d, h, p], cr.at[d, h, p], sib)

    def cross_from(d, h, p):
        zz = lax.rem(z + nz - h, nz) if d == 0 else lax.rem(z + h, nz)
        b = zz * 2 + (1 - c)
        return remote(piece(b, p), piece(b, p), cs.at[d, h, p], cr.at[d, h, p], sib)

    far = nz // 2
    sends = []

    def pieces(d, h):
        return (0, 1) if h < far else ((0,) if d == 0 else (1,))

    for p in (0, 1):
        for d in (0, 1):
            q = hop(d, 1, p)
            q.start()
            sends.append(q)
    for p in (0, 1):
        q = cross(mine, 0, 0, p)
        q.start()
        sends.append(q)

    def expert(blocks):
        xin = jnp.concatenate([rows[b] for b in blocks], axis=0)
        g = dot(xin, gw[...])
        u = dot(xin, uw[...])
        hval = (g * jax.nn.sigmoid(g) * u).astype(BF)
        for i, b in enumerate(blocks):
            hid[0, b] = hval[i * per : (i + 1) * per]

    def hswap(b, k):
        return remote(hid.at[0, b], hid.at[1, b], hs.at[k], hr_.at[k], sib)

    def blocks_of(h):
        if h == 0:
            return [(z * 2 + 0, 0), (z * 2 + 1, 1)]
        lo = lax.rem(z + nz - h, nz)
        hi = lax.rem(z + h, nz)
        if h == far:
            return [(lo * 2 + k, 4 * h - 2 + k) for k in (0, 1)]
        return [(lo * 2 + k, 4 * h - 2 + k) for k in (0, 1)] + [
            (hi * 2 + k, 4 * h + k) for k in (0, 1)
        ]

    def run(h):
        bl = blocks_of(h)
        expert([b for b, k in bl])
        for b, k in bl:
            q = hswap(b, k)
            q.start()
            sends.append(q)
        for b, k in bl:
            hswap(b, k).wait_recv()

    width = half // nsub

    def ring(d, s, j):
        to = right if d == 0 else left
        return remote(
            sbuf.at[d, s, :, pl.ds(j * width, width)],
            rbuf.at[d, s, :, pl.ds(j * width, width)],
            ss.at[d, s, j],
            rs.at[d, s, j],
            (y, x, to, c),
        )

    def own(d, s):
        zz = lax.rem(z + nz - 1 - s, nz) if d == 0 else lax.rem(z + 1 + s, nz)
        b = zz * 2 + d
        return dot(hid[0, b], dw[...]) + dot(hid[1, b], dsib[...])

    def own_pair(d, s):
        zz = lax.rem(z + nz - 1 - s, nz) if d == 0 else lax.rem(z + 1 + s, nz)
        b = zz * 2 + d
        return hid[0, b], hid[1, b]

    def partial(d, s):
        h0, h1 = own_pair(d, s)
        first = jnp.where(c == 0, 1, 0)
        del first
        return dot(h0, dw[...]) + dot(h1, dsib[...])

    def reduce_step(s):
        for d in range(2):
            val = partial(d, s)
            for j in range(nsub):
                cols = slice(j * width, (j + 1) * width)
                v = val[:, cols]
                if s > 0:
                    ring(d, s - 1, j).wait_recv()
                    v = v + rbuf[d, s - 1, :, cols].astype(F32)
                sbuf[d, s, :, cols] = v.astype(BF)
                q = ring(d, s, j)
                q.start()
                sends.append(q)

    for q in loads[:2]:
        q.wait()
    for p in (0, 1):
        cross_from(0, 0, p).wait_recv()
    run(0)
    loads[2].wait()
    wcopy.wait_recv()
    for h in range(1, far + 1):
        for p in (0, 1):
            for d in (0, 1):
                if p not in pieces(d, h):
                    continue
                b, q = got(d, h, p)
                q.wait_recv()
                if h + 1 <= far and p in pieces(d, h + 1):
                    f = hop(d, h + 1, p)
                    f.start()
                    sends.append(f)
                f = cross(b, d, h, p)
                f.start()
                sends.append(f)
        for p in (0, 1):
            for d in (0, 1):
                if p in pieces(d, h):
                    cross_from(d, h, p).wait_recv()
        run(h)
        reduce_step(h - 1)
    for s in range(far, nz - 1):
        reduce_step(s)
    for d in range(2):
        val = partial(d, nz - 1)
        tot = []
        for j in range(nsub):
            cols = slice(j * width, (j + 1) * width)
            ring(d, nz - 2, j).wait_recv()
            tot.append(val[:, cols] + rbuf[d, nz - 2, :, cols].astype(F32))
        tot = jnp.concatenate(tot, axis=1).astype(BF)
        for e in range(n):
            fin[d, e] = tot[2 * e : 2 * e + 2, :]
        for i, (ty, tx, t) in enumerate(others):
            q = remote(
                fin.at[d, t], out.at[c, me], fs.at[d, i], fr.at[c, me], (ty, tx, z, d)
            )
            q.start()
            sends.append(q)
    keep = remote(fin.at[1 - c, me], out.at[c, me], fs.at[0, n - 1], fr.at[c, me], sib)
    keep.start()
    sends.append(keep)
    out[c, me] = fin[c, me]
    for k in (0, 1):
        for ty, tx, t in others:
            remote(fin.at[0, t], out.at[k, t], fs.at[0, 0], fr.at[k, t], sib).wait_recv()
    remote(fin.at[0, me], out.at[1 - c, me], fs.at[0, 0], fr.at[1 - c, me], sib).wait_recv()
    for d, (ty, tx, t) in enumerate(others):
        remote(sent.at[t], inb.at[me], is_.at[d], ir.at[me], (ty, tx, z, c)).wait_send()
    wcopy.wait_send()
    for q in sends:
        q.wait_send()


def experts(sent, gate, up, down, ny, nx, nz, cid):
    n = ny * nx
    d_model, units = gate.shape
    half = d_model // 2
    per = 2 * n
    nsub = 2
    far = nz // 2
    dma = pltpu.SemaphoreType.DMA
    return pl.pallas_call(
        functools.partial(expert_kernel, ny, nx, nz, nsub),
        out_shape=jax.ShapeDtypeStruct((2, n, 2, half), BF),
        in_specs=[VM, ANY, ANY, ANY],
        out_specs=VM,
        scratch_shapes=[
            pltpu.VMEM((d_model, units), BF),
            pltpu.VMEM((d_model, units), BF),
            pltpu.VMEM((units, half), BF),
            pltpu.VMEM((units, half), BF),
            pltpu.VMEM((n, 2, d_model), BF),
            pltpu.VMEM((2 * nz, per, d_model), BF),
            pltpu.VMEM((2, 2 * nz, per, units), BF),
            pltpu.VMEM((2, nz - 1, per, half), BF),
            pltpu.VMEM((2, nz - 1, per, half), BF),
            pltpu.VMEM((2, n, 2, half), BF),
            dma((3,)),
            dma, dma,
            dma((n - 1,)), dma((n,)),
            dma((2, far + 1, 2)), dma((2, far + 1, 2)),
            dma((2, far + 1, 2)), dma((2, far + 1, 2)),
            dma((2 * nz,)), dma((2 * nz,)),
            dma((2, nz - 1, nsub)), dma((2, nz - 1, nsub)),
            dma((2, n)), dma((2, n)),
        ],
        compiler_params=pltpu.CompilerParams(
            collective_id=cid, has_side_effects=True, vmem_limit_bytes=LIMIT
        ),
        name="experts",
    )(sent, gate, up, down)


def normalize(rows, norm_gain):
    rows_f = rows.astype(F32)
    scaling = lax.rsqrt(jnp.mean(rows_f * rows_f, axis=1, keepdims=True) + 1e-06)
    return (rows_f * scaling * norm_gain[None, :]).astype(BF)


def route_weights(normed, group_router, expert_router, chosen, group_size):
    group_logits = dot(normed, group_router)
    expert_logits = dot(normed, expert_router)
    chosen_group = chosen[:, 0] // group_size
    margin = group_logits[:, 0] - group_logits[:, 1]
    own_margin = jnp.where(chosen_group == 0, margin, -margin)
    experts_iota = jnp.arange(expert_logits.shape[1], dtype=jnp.int32)
    picked = jnp.sum(
        jnp.where(
            chosen[:, :, None] == experts_iota[None, None, :], expert_logits[:, None, :], F32(0.0)
        ),
        axis=2,
    )
    return jax.nn.sigmoid(own_margin)[:, None] * jax.nn.sigmoid(picked - picked[:, ::-1])


def slot_table(chosen, expert_count, slots):
    flat_ids = chosen.reshape(-1)
    same = flat_ids[:, None] == flat_ids[None, :]
    at = jnp.arange(flat_ids.shape[0], dtype=jnp.int32)
    ranks = jnp.sum((same & (at[None, :] < at[:, None])).astype(jnp.int32), axis=1)
    return (flat_ids * slots + ranks).reshape(chosen.shape)


def per_device(
    residual_in, queries, keys, values, break_offset, doc_ids, out_weight, norm_gain,
    group_router, expert_router, expert_ids, gate_weight, up_weight, down_weight,
):
    ny, nx, nz = lax.axis_size("y"), lax.axis_size("x"), lax.axis_size("z")
    tok_dev = queries.shape[0]
    heads_dev = break_offset.shape[1]
    rows_dev, width = residual_in.shape
    experts_all = ny * nx
    own_begin = lax.axis_index(TP) * rows_dev
    aux = jnp.concatenate(
        [
            break_offset.T,
            doc_ids.astype(BF)[None, :],
            jnp.zeros((16 - heads_dev - 1, tok_dev), BF),
        ],
        axis=0,
    )
    kall, vall, aall, wsib = gather_keys(keys, values, aux, out_weight, ny, nx, 1)
    attended = attend(queries, kall, vall, aall, doc_ids.astype(F32)[:, None], nx)
    mixed_stream = project(attended, out_weight, wsib, residual_in, nz, 2)
    chosen = lax.dynamic_slice_in_dim(expert_ids, own_begin, rows_dev, 0)
    normed = normalize(mixed_stream, norm_gain)
    routes = route_weights(
        normed, group_router, expert_router, chosen, experts_all // GROUPS
    )
    slot_ids = slot_table(chosen, experts_all, 2)
    onehot = (
        jnp.arange(2 * experts_all, dtype=jnp.int32)[:, None, None] == slot_ids[None]
    ).sum(axis=2)
    sent = dot(onehot.astype(BF), normed).astype(BF).reshape(experts_all, 2, width)
    back = experts(sent, gate_weight[0], up_weight[0], down_weight[0], ny, nx, nz, 3)
    back = back.transpose(1, 2, 0, 3).reshape(2 * experts_all, width)
    expert_out = jnp.take(back, slot_ids.reshape(-1), axis=0).reshape(rows_dev, 2, width)
    mixture = jnp.sum(routes[:, :, None] * expert_out.astype(F32), axis=1)
    return (mixed_stream.astype(F32) + mixture).astype(BF)


def solution(mesh):
    n = mesh.shape["sp"]
    side = round(n**0.5)
    finer = Mesh(
        mesh.devices.reshape(side, n // side, mesh.shape["tp"] // 2, 2), AXES
    )
    in_specs = (
        P(SP + TP, None),
        P(SP, TP),
        P(SP, TP),
        P(SP, TP),
        P(SP, TP),
        P(SP),
        P(TP, None),
        P(),
        P(),
        P(),
        P(SP, None),
        P(SP, None, TP),
        P(SP, None, TP),
        P(SP, TP, None),
    )
    return jax.shard_map(
        per_device, mesh=finer, in_specs=in_specs, out_specs=P(SP + TP, None), check_vma=False
    )
```

```python
import functools

import jax
import jax.numpy as jnp
from jax import lax
from jax.experimental import pallas as pl
from jax.experimental.pallas import tpu as pltpu
from jax.sharding import Mesh
from jax.sharding import PartitionSpec as P

HEAD_DIM = 64
GROUPS = 2
DOC_MOST = 2560
KB = 256
BAND = DOC_MOST // KB
NEG = -1e30
SUM_PIECES = 2
ROW_PIECES = 4
BACK_PIECES = 4
MESH = pl.DeviceIdType.MESH
AXES = ("y", "x", "z", "c")
SP = ("y", "x")
TP = ("z", "c")
VM = pl.BlockSpec(memory_space=pltpu.VMEM)
ANY = pl.BlockSpec(memory_space=pl.ANY)
BF = jnp.bfloat16
F32 = jnp.float32
LIMIT = 60 * 1024 * 1024


def dot(a, b):
    return jnp.dot(a, b, preferred_element_type=F32)


def dot_t(a, b):
    return lax.dot_general(a, b, (((1,), (1,)), ((), ())), preferred_element_type=F32)


def iota(shape, axis):
    return lax.broadcasted_iota(jnp.int32, shape, axis)


def remote(src, dst, ss, rs, to):
    return pltpu.make_async_remote_copy(
        src_ref=src, dst_ref=dst, send_sem=ss, recv_sem=rs, device_id=to, device_id_type=MESH
    )


def attend_block(diag, q, kb, vb, ab, qd, acc, st, later):
    heads = q.shape[1] // HEAD_DIM
    rows = q.shape[0]
    live = ab[heads : heads + 1, :].astype(F32) == qd[...]
    if diag:
        live = live & (iota((rows, KB), 1) < iota((rows, KB), 0))
    for h in range(heads):
        hs = slice(h * HEAD_DIM, (h + 1) * HEAD_DIM)
        s = dot_t(q[:, hs], kb[:, hs]) + ab[h : h + 1, :].astype(F32)
        s = jnp.where(live, s, NEG)
        go = jnp.maximum(s, 0.0) + jnp.log(1.0 + jnp.exp(-jnp.abs(s)))
        hi = go.astype(BF)
        lo = (go - hi.astype(F32)).astype(BF)
        within = dot(hi, later[...]) + dot(lo, later[...])
        wt = jnp.exp(s - go - within).astype(BF)
        o = dot(wt, vb[:, hs])
        total = jnp.sum(go, axis=1, keepdims=True)
        if diag:
            acc[:, hs] = o
            st[h] = total
        else:
            before = st[h]
            acc[:, hs] = acc[:, hs] + jnp.exp(-before) * o
            st[h] = before + total


def layer_kernel(
    dims,
    res, q, k, v, off, doc, w, gain, grp, exr, ids, gate, up, down,
    out,
    kall, vall, aall, auxo, later, qs, qd, acc, st,
    wown, wsib, att, pair, part, sbb, rbb, xbuf, ybuf, mixed,
    sent, inb, rows, gw, uw, dw, dsib, hid, partc, sbc, rbc, fin, ret, back, grw, exw,
    lsem, ks, kr, vs, vr, as_, ar, ws, wr, ds, dr, bs, br, es, er,
    is_, ir, gs, gr, cs, cr, hs_, hr_, ss, rs, fs, fr,
):
    ny, nx, nz = dims
    y, x, z, c = (lax.axis_index(a) for a in AXES)
    me = y * nx + x
    n = ny * nx
    sib = (y, x, z, 1 - c)
    right = (y, x, lax.rem(z + 1, nz), c)
    left = (y, x, lax.rem(z + nz - 1, nz), c)
    half = wown.shape[1]
    heads = off.shape[1]
    own_half = pl.ds(pl.multiple_of(c * half, half), half)
    other_half = pl.ds(pl.multiple_of((1 - c) * half, half), half)
    far = nz // 2
    sends = []

    def start(q_):
        q_.start()
        sends.append(q_)

    loads = [
        pltpu.make_async_copy(w.at[:, own_half], wown, lsem.at[0]),
        pltpu.make_async_copy(gate, gw, lsem.at[1]),
        pltpu.make_async_copy(up, uw, lsem.at[2]),
        pltpu.make_async_copy(down.at[:, own_half], dw, lsem.at[3]),
        pltpu.make_async_copy(grp, grw, lsem.at[4]),
        pltpu.make_async_copy(exr, exw, lsem.at[5]),
    ]
    for a in loads:
        a.start()
    others = []
    for d in range(1, n):
        t = lax.rem(me + d, n)
        others.append((lax.div(t, nx), lax.rem(t, nx), t))
    peers = [(ty, tx, z, c) for ty, tx, t in others]
    peers += [(ty, tx, z, 1 - c) for ty, tx, t in others]
    peers += [right, left, sib]
    bar = pltpu.get_barrier_semaphore()
    for p in peers:
        pl.semaphore_signal(bar, inc=1, device_id=p, device_id_type=MESH)

    eye = (iota((KB, KB), 0) == iota((KB, KB), 1)).astype(BF)
    later[...] = (iota((KB, KB), 0) > iota((KB, KB), 1)).astype(BF)
    docf = doc[...].astype(F32)
    qd[...] = jnp.sum(jnp.where(eye > 0, docf, 0.0), axis=1, keepdims=True)
    offs = []
    for h in range(heads):
        col = off[:, h : h + 1].astype(F32)
        offs.append(jnp.sum(jnp.where(eye > 0, col, 0.0), axis=0, keepdims=True))
    pad = jnp.zeros((auxo.shape[0] - heads - 1, KB), F32)
    auxo[...] = jnp.concatenate(offs + [docf, pad], axis=0).astype(BF)
    qs[...] = q[...] * BF(HEAD_DIM**-0.5)
    pl.semaphore_wait(bar, len(peers))

    xs = [lax.rem(x + d, nx) for d in range(1, nx)]
    ys = [lax.rem(y + d, ny) for d in range(1, ny)]
    xb = [lax.rem(x + nx - d, nx) for d in range(1, nx)]
    yb = [lax.rem(y + ny - d, ny) for d in range(1, ny)]

    def used(b, j):
        return (j > b) & (j - b <= BAND)

    def k_first(src, dst):
        return (dst > src) | (y < ny - 1)

    def v_first(dst, src, col):
        return (dst > src) & (nx * (dst - src) - col <= BAND)

    def kcopy(b, src, asrc, i, to):
        return (
            remote(src, kall.at[b], ks.at[i], kr.at[b], to),
            remote(asrc, aall.at[b], as_.at[i], ar.at[b], to),
        )

    def vcopy(b, src, i, to):
        return (remote(src, vall.at[b], vs.at[i], vr.at[b], to),)

    plan = []

    def send(cond, copies):
        plan.append((cond, copies))

        @pl.when(cond)
        def _():
            for a in copies:
                a.start()

    def arrive(cond, copies):
        @pl.when(cond)
        def _():
            for a in copies:
                a.wait_recv()

    nk = nv = 0
    for a in xs:
        send(k_first(x, a), kcopy(me, k, auxo, nk, (y, a, z, c)))
        nk += 1
    for a in ys:
        send(v_first(a, y, x), vcopy(me, v, nv, (a, x, z, c)))
        nv += 1
    for a in ys:
        send(used(me, a * nx + x), kcopy(me, k, auxo, nk, (a, x, z, c)))
        nk += 1
    for a in xs:
        send(used(me, y * nx + a), vcopy(me, v, nv, (y, a, z, c)))
        nv += 1
    start(remote(w.at[:, other_half], wsib, ws.at[0], wr.at[0], sib))
    start(remote(down.at[:, other_half], dsib, ws.at[1], wr.at[1], sib))

    attend_block(True, qs, k, v, auxo, qd, acc, st, later)

    firsts = []
    for i in range(max(nx, ny) - 1):
        if i < nx - 1:
            b = y * nx + xb[i]
            got = k_first(xb[i], x)
            arrive(got, kcopy(b, k, auxo, 0, sib))
            for a in ys:
                send(got & used(b, a * nx + x), kcopy(b, kall.at[b], aall.at[b], nk, (a, x, z, c)))
                nk += 1
        if i < ny - 1:
            b = yb[i] * nx + x
            got = v_first(y, yb[i], x)
            arrive(got, vcopy(b, v, 0, sib))
            for a in xs:
                send(got & used(b, y * nx + a), vcopy(b, vall.at[b], nv, (y, a, z, c)))
                nv += 1
    del firsts

    def step(t, carry):
        b = me - t
        by = lax.div(b, nx)
        bx = lax.rem(b, nx)

        @pl.when(by != y)
        def _():
            for a in kcopy(b, k, auxo, 0, sib):
                a.wait_recv()

        @pl.when(bx != x)
        def _():
            for a in vcopy(b, v, 0, sib):
                a.wait_recv()

        attend_block(
            False, qs, kall.at[b], vall.at[b], aall.at[b], qd, acc, st, later
        )
        return carry

    lax.fori_loop(1, jnp.minimum(me, BAND) + 1, step, 0)
    att[...] = acc[...].astype(BF)
    swap = remote(att, pair, ds, dr, sib)
    start(swap)

    def ring_sum(own, sbuf, rbuf, s_sem, r_sem, np_, hr, last):
        def move(d, s, p):
            ref = (d, s, pl.ds(p * hr, hr))
            return remote(
                sbuf.at[ref], rbuf.at[ref], s_sem.at[d, s, p], r_sem.at[d, s, p],
                right if d == 0 else left,
            )

        def half_of(d):
            return range(np_ // 2) if d == 0 else range(np_ // 2, np_)

        for s in range(far):
            for i in range(np_ // 2 if s == 0 else np_):
                for d in range(2):
                    order = list(half_of(d)) + ([] if s == 0 else list(half_of(1 - d)))
                    p = order[i]
                    dist = far - s
                    zz = lax.rem(z + dist, nz) if d == 0 else lax.rem(z + nz - dist, nz)
                    val = own(zz, p)
                    if s > 1 or (s == 1 and p in half_of(d)):
                        move(d, s - 1, p).wait_recv()
                        val = val + rbuf[d, s - 1, p * hr : (p + 1) * hr, :].astype(F32)
                    sbuf[d, s, p * hr : (p + 1) * hr, :] = val.astype(BF)
                    start(move(d, s, p))
        for i in range(np_):
            p = i
            for d in range(2):
                move(d, far - 1, p).wait_recv()
            tot = own(z, p)
            for d in range(2):
                tot = tot + rbuf[d, far - 1, p * hr : (p + 1) * hr, :].astype(F32)
            last(p, tot)

    chunk = part.shape[0] // nz
    hr = chunk // SUM_PIECES
    loads[0].wait()
    part[...] = dot(att[...], wown[...])
    remote(w.at[:, other_half], wsib, ws.at[0], wr.at[0], sib).wait_recv()
    swap.wait_recv()
    part[...] += dot(pair[...], wsib[...])

    def own_b(zz, p):
        return part[pl.ds(pl.multiple_of(zz * chunk + p * hr, hr), hr), :]

    crow = chunk // 2

    def last_b(p, tot):
        for i in range(max(1, hr // crow)):
            r = p * hr + i * crow if hr >= crow else p * hr
            cnt = min(hr, crow)
            core = r // crow
            at = r % crow
            piece = tot[i * crow : i * crow + cnt] if hr >= crow else tot

            @pl.when(c == core)
            def _():
                ybuf[c, at : at + cnt, :] = piece

            @pl.when(c != core)
            def _():
                xbuf[at : at + cnt, :] = piece

    ring_sum(own_b, sbb, rbb, bs, br, SUM_PIECES, hr, last_b)
    trade = remote(xbuf, ybuf.at[c], es, er, sib)
    start(trade)
    remote(xbuf, ybuf.at[1 - c], es, er, sib).wait_recv()
    lo = res[:, :half].astype(F32) + ybuf[0]
    hi = res[:, half:].astype(F32) + ybuf[1]
    mlo, mhi = lo.astype(BF), hi.astype(BF)
    mixed[:, :half] = mlo
    mixed[:, half:] = mhi
    lo, hi = mlo.astype(F32), mhi.astype(F32)
    mean = (
        jnp.sum(lo * lo, axis=1, keepdims=True) + jnp.sum(hi * hi, axis=1, keepdims=True)
    ) / (2 * half)
    scale = lax.rsqrt(mean + 1e-06)
    nlo = (lo * scale * gain[:, :half]).astype(BF)
    nhi = (hi * scale * gain[:, half:]).astype(BF)

    tok = res.shape[0]
    chosen = ids[pl.ds(pl.multiple_of((z * 2 + c) * tok, tok), tok), :]
    eye16 = iota((tok, tok), 0) == iota((tok, tok), 1)
    trow = [
        jnp.sum(jnp.where(eye16, chosen[:, i : i + 1], 0), axis=0, keepdims=True)
        for i in range(2)
    ]
    slot = iota((2 * n, tok), 0)
    expert_of = lax.div(slot, 2)
    named = ((trow[0] == expert_of) | (trow[1] == expert_of)).astype(F32)
    earlier = (iota((tok, tok), 0) < iota((tok, tok), 1)).astype(BF)
    rank = dot(named.astype(BF), earlier)
    odd = lax.rem(slot, 2).astype(F32)
    pick = jnp.where(rank == odd, named, 0.0).astype(BF)
    slo = dot(pick, nlo).astype(BF)
    shi = dot(pick, nhi).astype(BF)
    for e in range(n):
        sent[e, :, :half] = slo[2 * e : 2 * e + 2, :]
        sent[e, :, half:] = shi[2 * e : 2 * e + 2, :]

    for d, (ty, tx, t) in enumerate(others):
        start(remote(sent.at[t], inb.at[me], is_.at[d], ir.at[me], (ty, tx, z, c)))
    inb[me] = sent[me]

    normed = jnp.concatenate([nlo, nhi], axis=1)
    loads[4].wait()
    loads[5].wait()
    glog = dot(normed, grw[...])
    elog = dot(normed, exw[...])
    margin = glog[:, 0:1] - glog[:, 1:2]
    own_margin = jnp.where(chosen[:, 0:1] < n // GROUPS, margin, -margin)
    share = jax.nn.sigmoid(own_margin)
    eid = iota((tok, n), 1)
    picked = [
        jnp.sum(jnp.where(chosen[:, i : i + 1] == eid, elog, 0.0), axis=1, keepdims=True)
        for i in range(2)
    ]
    route = [share * jax.nn.sigmoid(picked[i] - picked[1 - i]) for i in range(2)]
    slot_c = iota((tok, 2 * n), 1)
    exp_c = lax.div(slot_c, 2)
    is_k = [chosen[:, i : i + 1] == exp_c for i in range(2)]
    named_c = (is_k[0] | is_k[1]).astype(BF)
    before = (iota((tok, tok), 1) < iota((tok, tok), 0)).astype(BF)
    rank_c = dot(before, named_c)
    odd_c = lax.rem(slot_c, 2).astype(F32)
    take = [
        jnp.where(is_k[i] & (rank_c == odd_c), 1.0, 0.0).astype(BF) for i in range(2)
    ]

    for ty, tx, t in others:
        remote(sent.at[t], inb.at[t], is_.at[0], ir.at[t], sib).wait_recv()
    mine = z * 2 + c
    for e in range(n):
        rows[mine, 2 * e : 2 * e + 2, :] = inb[e]

    per = rows.shape[1]
    hb = per // ROW_PIECES

    def piece(b, p):
        return rows.at[b, pl.ds(p * hb, hb), :]

    def from_chip(d, h):
        return lax.rem(z + nz - h, nz) if d == 0 else lax.rem(z + h, nz)

    def hop(d, h, p):
        b = from_chip(d, h - 1) * 2 + c
        return remote(
            piece(b, p), piece(b, p), gs.at[d, h, p], gr.at[d, h, p], right if d == 0 else left
        )

    def got_hop(d, h, p):
        b = from_chip(d, h) * 2 + c
        return remote(piece(b, p), piece(b, p), gs.at[d, h, p], gr.at[d, h, p], sib)

    def cross(d, h, p, core):
        b = from_chip(d, h) * 2 + core
        return remote(piece(b, p), piece(b, p), cs.at[d, h, p], cr.at[d, h, p], sib)

    def pieces(d, h):
        if h < far:
            return list(range(ROW_PIECES))
        hp = ROW_PIECES // 2
        return list(range(hp)) if d == 0 else list(range(hp, ROW_PIECES))

    def order(d):
        hp = ROW_PIECES // 2
        a = list(range(hp))
        b = list(range(hp, ROW_PIECES))
        return a + b if d == 0 else b + a

    for i in range(ROW_PIECES):
        for d in (0, 1):
            start(hop(d, 1, order(d)[i]))
    for p in range(ROW_PIECES):
        start(cross(0, 0, p, c))

    def blocks_of(h):
        if h == 0:
            return [(z * 2 + i, i) for i in (0, 1)]
        lo_ = from_chip(0, h)
        hi_ = from_chip(1, h)
        if h == far:
            return [(lo_ * 2 + i, 4 * h - 2 + i) for i in (0, 1)]
        return [(lo_ * 2 + i, 4 * h - 2 + i) for i in (0, 1)] + [
            (hi_ * 2 + i, 4 * h + i) for i in (0, 1)
        ]

    def hswap(b, i):
        return remote(hid.at[0, b], hid.at[1, b], hs_.at[i], hr_.at[i], sib)

    def run(h):
        for d in (0, 1):
            if h == 0 and d == 1:
                continue
            for p in pieces(d, h):
                cross(d, h, p, 1 - c).wait_recv()
        bl = blocks_of(h)
        xin = jnp.concatenate([rows[b] for b, i in bl], axis=0)
        g = dot(xin, gw[...])
        u = dot(xin, uw[...])
        hv = (g * jax.nn.sigmoid(g) * u).astype(BF)
        for j, (b, i) in enumerate(bl):
            hid[0, b] = hv[j * per : (j + 1) * per]
            start(hswap(b, i))

    def finish(h):
        bl = blocks_of(h)
        for b, i in bl:
            hswap(b, i).wait_recv()
        h0 = jnp.concatenate([hid[0, b] for b, i in bl], axis=0)
        h1 = jnp.concatenate([hid[1, b] for b, i in bl], axis=0)
        val = dot(h0, dw[...]) + dot(h1, dsib[...])
        for j, (b, i) in enumerate(bl):
            partc[b] = val[j * per : (j + 1) * per]

    loads[1].wait()
    loads[2].wait()
    for h in range(1, far + 1):
        for i in range(ROW_PIECES):
            for d in (0, 1):
                p = order(d)[i]
                if p not in pieces(d, h):
                    continue
                got_hop(d, h, p).wait_recv()
                if h + 1 <= far and p in pieces(d, h + 1):
                    start(hop(d, h + 1, p))
                start(cross(d, h, p, c))
            if i == 0:
                run(h - 1)
                if h == 1:
                    loads[3].wait()
                    remote(down.at[:, other_half], dsib, ws.at[1], wr.at[1], sib).wait_recv()
            if i == 1:
                finish(h - 1)
    run(far)
    finish(far)

    chunk_c = 2 * per
    hc = chunk_c // BACK_PIECES

    def own_c(zz, p):
        b = zz * 2 + (p * hc) // per
        return partc[b, (p * hc) % per : (p * hc) % per + hc, :]

    def last_c(p, tot):
        core = (p * hc) // per
        e0 = ((p * hc) % per) // 2
        tb = tot.astype(BF)
        for e in range(hc // 2):
            t = e0 + e
            fin[core, t] = tb[2 * e : 2 * e + 2, :]
            ty, tx = t // nx, t % nx

            @pl.when(me != t)
            def _(t=t, ty=ty, tx=tx):
                remote(
                    fin.at[core, t], ret.at[c, me], fs.at[core, t], fr.at[c, me], (ty, tx, z, core)
                ).start()

            @pl.when((me == t) & (c != core))
            def _(t=t):
                remote(
                    fin.at[core, t], ret.at[c, me], fs.at[core, t], fr.at[c, me], sib
                ).start()

    ring_sum(own_c, sbc, rbc, ss, rs, BACK_PIECES, hc, last_c)
    ret[c, me] = fin[c, me]
    for i in (0, 1):
        for t in range(n):

            @pl.when((me != t) | (c != i))
            def _(t=t, i=i):
                remote(fin.at[0, t], ret.at[i, t], fs.at[0, t], fr.at[i, t], sib).wait_recv()

            back[2 * t : 2 * t + 2, i * half : (i + 1) * half] = ret[i, t]
    for i in range(2):
        cols = slice(i * half, (i + 1) * half)
        bk = back[:, cols]
        mix = route[0] * dot(take[0], bk) + route[1] * dot(take[1], bk)
        out[:, cols] = (mixed[:, cols].astype(F32) + mix).astype(BF)

    for cond, copies in plan:

        @pl.when(cond)
        def _(copies=copies):
            for a in copies:
                a.wait_send()

    for core in (0, 1):
        for t in range(n):

            @pl.when((me != t) | (c != core))
            def _(t=t, core=core):
                remote(
                    fin.at[core, t], ret.at[c, me], fs.at[core, t], fr.at[c, me], sib
                ).wait_send()

    for a in sends:
        a.wait_send()


def per_device(
    residual_in, queries, keys, values, break_offset, doc_ids, out_weight, norm_gain,
    group_router, expert_router, expert_ids, gate_weight, up_weight, down_weight,
):
    ny, nx, nz = lax.axis_size("y"), lax.axis_size("x"), lax.axis_size("z")
    n = ny * nx
    rows, att = queries.shape
    tok, width = residual_in.shape
    half = width // 2
    heads = break_offset.shape[1]
    gate, up, down = gate_weight[0], up_weight[0], down_weight[0]
    units = gate.shape[1]
    per = 2 * n
    far = nz // 2
    sends = (nx - 1) + (ny - 1) + (nx - 1) * (ny - 1)
    dma = pltpu.SemaphoreType.DMA
    vm = pltpu.VMEM
    scratch = [
        vm((n, rows, att), BF), vm((n, rows, att), BF), vm((n, 16, rows), BF), vm((16, rows), BF),
        vm((KB, KB), BF), vm((rows, att), BF), vm((rows, 1), F32), vm((rows, att), F32),
        vm((heads, rows, 1), F32),
        vm((att, half), BF), vm((att, half), BF), vm((rows, att), BF), vm((rows, att), BF),
        vm((rows, half), F32),
        vm((2, far, rows // nz, half), BF), vm((2, far, rows // nz, half), BF),
        vm((tok, half), F32), vm((2, tok, half), F32), vm((tok, width), BF),
        vm((n, 2, width), BF), vm((n, 2, width), BF), vm((2 * nz, per, width), BF),
        vm((width, units), BF), vm((width, units), BF), vm((units, half), BF),
        vm((units, half), BF),
        vm((2, 2 * nz, per, units), BF), vm((2 * nz, per, half), F32),
        vm((2, far, 2 * per, half), BF), vm((2, far, 2 * per, half), BF),
        vm((2, n, 2, half), BF), vm((2, n, 2, half), BF), vm((per, width), BF),
        vm(group_router.shape, BF), vm(expert_router.shape, BF),
        dma((6,)),
        dma((sends,)), dma((n,)), dma((sends,)), dma((n,)), dma((sends,)), dma((n,)),
        dma((2,)), dma((2,)), dma, dma,
        dma((2, far, SUM_PIECES)), dma((2, far, SUM_PIECES)), dma, dma,
        dma((n - 1,)), dma((n,)),
        dma((2, far + 1, ROW_PIECES)), dma((2, far + 1, ROW_PIECES)),
        dma((2, far + 1, ROW_PIECES)), dma((2, far + 1, ROW_PIECES)),
        dma((2 * nz,)), dma((2 * nz,)),
        dma((2, far, BACK_PIECES)), dma((2, far, BACK_PIECES)),
        dma((2, n)), dma((2, n)),
    ]
    return pl.pallas_call(
        functools.partial(layer_kernel, (ny, nx, nz)),
        out_shape=jax.ShapeDtypeStruct(residual_in.shape, BF),
        in_specs=[VM] * 6 + [ANY, VM, ANY, ANY, VM, ANY, ANY, ANY],
        out_specs=VM,
        scratch_shapes=scratch,
        compiler_params=pltpu.CompilerParams(
            collective_id=1, has_side_effects=True, vmem_limit_bytes=LIMIT
        ),
        name="layer",
    )(
        residual_in, queries, keys, values, break_offset, doc_ids[None, :], out_weight,
        norm_gain[None, :], group_router, expert_router, expert_ids, gate, up, down,
    )


def solution(mesh):
    n = mesh.shape["sp"]
    side = round(n**0.5)
    finer = Mesh(mesh.devices.reshape(side, n // side, mesh.shape["tp"] // 2, 2), AXES)
    in_specs = (
        P(SP + TP, None),
        P(SP, TP),
        P(SP, TP),
        P(SP, TP),
        P(SP, TP),
        P(SP),
        P(TP, None),
        P(),
        P(),
        P(),
        P(SP, None),
        P(SP, None, TP),
        P(SP, None, TP),
        P(SP, TP, None),
    )
    return jax.shard_map(
        per_device, mesh=finer, in_specs=in_specs, out_specs=P(SP + TP, None), check_vma=False
    )
```

```python
import functools

import jax
import jax.numpy as jnp
from jax import lax
from jax.experimental import pallas as pl
from jax.experimental.pallas import tpu as pltpu
from jax.sharding import Mesh
from jax.sharding import PartitionSpec as P

HEAD_DIM = 64
GROUPS = 2
DOC_MOST = 2560
KB = 256
BAND = DOC_MOST // KB
NEG = -1e30
SUM_PIECES = 2
ROW_PIECES = 4
BACK_PIECES = 4
MESH = pl.DeviceIdType.MESH
AXES = ("y", "x", "z", "c")
SP = ("y", "x")
TP = ("z", "c")
VM = pl.BlockSpec(memory_space=pltpu.VMEM)
ANY = pl.BlockSpec(memory_space=pl.ANY)
BF = jnp.bfloat16
F32 = jnp.float32
LIMIT = 60 * 1024 * 1024


def dot(a, b):
    return jnp.dot(a, b, preferred_element_type=F32)


def dot_t(a, b):
    return lax.dot_general(a, b, (((1,), (1,)), ((), ())), preferred_element_type=F32)


def iota(shape, axis):
    return lax.broadcasted_iota(jnp.int32, shape, axis)


def remote(src, dst, ss, rs, to):
    return pltpu.make_async_remote_copy(
        src_ref=src, dst_ref=dst, send_sem=ss, recv_sem=rs, device_id=to, device_id_type=MESH
    )


def attend_block(diag, q, kb, vb, ab, qd, acc, st, later):
    heads = range(q.shape[1] // HEAD_DIM)
    rows = q.shape[0]
    cols = [slice(h * HEAD_DIM, (h + 1) * HEAD_DIM) for h in heads]
    scores = [dot_t(q[:, cols[h]], kb[:, cols[h]]) for h in heads]
    live = ab[len(heads) : len(heads) + 1, :].astype(F32) == qd[...]
    if diag:
        live = live & (iota((rows, KB), 1) < iota((rows, KB), 0))
    log_w, total = [], []
    for h in heads:
        s = jnp.where(live, scores[h] + ab[h : h + 1, :].astype(F32), NEG)
        go = jnp.maximum(s, 0.0) + jnp.log(1.0 + jnp.exp(-jnp.abs(s)))
        hi = go.astype(BF)
        lo = (go - hi.astype(F32)).astype(BF)
        total.append(jnp.sum(go, axis=1, keepdims=True))
        log_w.append((s - go, dot(hi, later[...]) + dot(lo, later[...])))
    for h in heads:
        o = dot(jnp.exp(log_w[h][0] - log_w[h][1]).astype(BF), vb[:, cols[h]])
        if diag:
            acc[:, cols[h]] = o
            st[h] = total[h]
        else:
            before = st[h]
            acc[:, cols[h]] = acc[:, cols[h]] + jnp.exp(-before) * o
            st[h] = before + total[h]


def layer_kernel(
    dims,
    res_, q_, k_, v_, off_, doc_, w, gain_, grp, exr, ids_, gate, up, down,
    out,
    res, q, k, v, off, doc, gain, ids,
    kall, vall, aall, auxo, later, qs, qd, acc, st,
    wown, wsib, att, pair, part, sbb, rbb, xbuf, ybuf, mixed,
    sent, inb, rows, gw, uw, dw, dsib, hid, partc, sbc, rbc, fin, ret, back, grw, exw,
    lsem, ks, kr, vs, vr, as_, ar, ws, wr, ds, dr, bs, br, es, er,
    is_, ir, gs, gr, cs, cr, hs_, hr_, ss, rs, fs, fr,
):
    ny, nx, nz = dims
    y, x, z, c = (lax.axis_index(a) for a in AXES)
    me = y * nx + x
    n = ny * nx
    sib = (y, x, z, 1 - c)
    right = (y, x, lax.rem(z + 1, nz), c)
    left = (y, x, lax.rem(z + nz - 1, nz), c)
    half = wown.shape[1]
    heads = off.shape[0]
    own_half = pl.ds(pl.multiple_of(c * half, half), half)
    other_half = pl.ds(pl.multiple_of((1 - c) * half, half), half)
    far = nz // 2
    sends = []

    def start(q_):
        q_.start()
        sends.append(q_)

    others = []
    for d in range(1, n):
        t = lax.rem(me + d, n)
        others.append((lax.div(t, nx), lax.rem(t, nx), t))
    peers = [(ty, tx, z, c) for ty, tx, t in others]
    peers += [(ty, tx, z, 1 - c) for ty, tx, t in others]
    peers += [right, left, sib]
    bar = pltpu.get_barrier_semaphore()
    for p in peers:
        pl.semaphore_signal(bar, inc=1, device_id=p, device_id_type=MESH)
    small = [
        pltpu.make_async_copy(a, b, lsem.at[6 + i])
        for i, (a, b) in enumerate(
            [(off_, off), (doc_, doc), (k_, k), (v_, v), (q_, q), (ids_, ids), (gain_, gain), (res_, res)]
        )
    ]
    loads = [
        pltpu.make_async_copy(w.at[:, own_half], wown, lsem.at[0]),
        pltpu.make_async_copy(gate, gw, lsem.at[1]),
        pltpu.make_async_copy(up, uw, lsem.at[2]),
        pltpu.make_async_copy(down.at[:, own_half], dw, lsem.at[3]),
        pltpu.make_async_copy(grp, grw, lsem.at[4]),
        pltpu.make_async_copy(exr, exw, lsem.at[5]),
    ]
    for a in small + loads:
        a.start()

    later[...] = (iota((KB, KB), 0) > iota((KB, KB), 1)).astype(BF)
    for a in small:
        a.wait()
    docf = doc[...].astype(F32)
    eye = iota((KB, KB), 0) == iota((KB, KB), 1)
    qd[...] = jnp.sum(jnp.where(eye, docf, 0.0), axis=1, keepdims=True)
    pad = jnp.zeros((auxo.shape[0] - heads - 1, KB), F32)
    auxo[...] = jnp.concatenate([off[...].astype(F32), docf, pad], axis=0).astype(BF)
    qs[...] = q[...] * BF(HEAD_DIM**-0.5)
    pl.semaphore_wait(bar, len(peers))

    xs = [lax.rem(x + d, nx) for d in range(1, nx)]
    ys = [lax.rem(y + d, ny) for d in range(1, ny)]
    xb = [lax.rem(x + nx - d, nx) for d in range(1, nx)]
    yb = [lax.rem(y + ny - d, ny) for d in range(1, ny)]

    def used(b, j):
        return (j > b) & (j - b <= BAND)

    def k_first(src, dst):
        return (dst > src) | (y < ny - 1)

    def v_first(dst, src, col):
        return (dst > src) & (nx * (dst - src) - col <= BAND)

    def kcopy(b, src, asrc, i, to):
        return (
            remote(src, kall.at[b], ks.at[i], kr.at[b], to),
            remote(asrc, aall.at[b], as_.at[i], ar.at[b], to),
        )

    def vcopy(b, src, i, to):
        return (remote(src, vall.at[b], vs.at[i], vr.at[b], to),)

    plan = []

    def send(cond, copies):
        plan.append((cond, copies))

        @pl.when(cond)
        def _():
            for a in copies:
                a.start()

    def arrive(cond, copies):
        @pl.when(cond)
        def _():
            for a in copies:
                a.wait_recv()

    nk = nv = 0
    for a in xs:
        send(k_first(x, a), kcopy(me, k, auxo, nk, (y, a, z, c)))
        nk += 1
    for a in ys:
        send(v_first(a, y, x), vcopy(me, v, nv, (a, x, z, c)))
        nv += 1
    for a in ys:
        send(used(me, a * nx + x), kcopy(me, k, auxo, nk, (a, x, z, c)))
        nk += 1
    for a in xs:
        send(used(me, y * nx + a), vcopy(me, v, nv, (y, a, z, c)))
        nv += 1
    start(remote(w.at[:, other_half], wsib, ws.at[0], wr.at[0], sib))
    start(remote(down.at[:, other_half], dsib, ws.at[1], wr.at[1], sib))

    attend_block(True, qs, k, v, auxo, qd, acc, st, later)

    firsts = []
    for i in range(max(nx, ny) - 1):
        if i < nx - 1:
            b = y * nx + xb[i]
            got = k_first(xb[i], x)
            arrive(got, kcopy(b, k, auxo, 0, sib))
            for a in ys:
                send(got & used(b, a * nx + x), kcopy(b, kall.at[b], aall.at[b], nk, (a, x, z, c)))
                nk += 1
        if i < ny - 1:
            b = yb[i] * nx + x
            got = v_first(y, yb[i], x)
            arrive(got, vcopy(b, v, 0, sib))
            for a in xs:
                send(got & used(b, y * nx + a), vcopy(b, vall.at[b], nv, (y, a, z, c)))
                nv += 1
    del firsts

    def step(t, carry):
        b = me - t
        by = lax.div(b, nx)
        bx = lax.rem(b, nx)

        @pl.when(by != y)
        def _():
            for a in kcopy(b, k, auxo, 0, sib):
                a.wait_recv()

        @pl.when(bx != x)
        def _():
            for a in vcopy(b, v, 0, sib):
                a.wait_recv()

        attend_block(
            False, qs, kall.at[b], vall.at[b], aall.at[b], qd, acc, st, later
        )
        return carry

    lax.fori_loop(1, jnp.minimum(me, BAND) + 1, step, 0)
    att[...] = acc[...].astype(BF)
    swap = remote(att, pair, ds, dr, sib)
    start(swap)

    def ring_sum(own, sbuf, rbuf, s_sem, r_sem, np_, hr, last):
        def move(d, s, p):
            ref = (d, s, pl.ds(p * hr, hr))
            return remote(
                sbuf.at[ref], rbuf.at[ref], s_sem.at[d, s, p], r_sem.at[d, s, p],
                right if d == 0 else left,
            )

        def half_of(d):
            return range(np_ // 2) if d == 0 else range(np_ // 2, np_)

        for s in range(far):
            for i in range(np_ // 2 if s == 0 else np_):
                for d in range(2):
                    order = list(half_of(d)) + ([] if s == 0 else list(half_of(1 - d)))
                    p = order[i]
                    dist = far - s
                    zz = lax.rem(z + dist, nz) if d == 0 else lax.rem(z + nz - dist, nz)
                    val = own(zz, p)
                    if s > 1 or (s == 1 and p in half_of(d)):
                        move(d, s - 1, p).wait_recv()
                        val = val + rbuf[d, s - 1, p * hr : (p + 1) * hr, :].astype(F32)
                    sbuf[d, s, p * hr : (p + 1) * hr, :] = val.astype(BF)
                    start(move(d, s, p))
        for i in range(np_):
            p = i
            for d in range(2):
                move(d, far - 1, p).wait_recv()
            tot = own(z, p)
            for d in range(2):
                tot = tot + rbuf[d, far - 1, p * hr : (p + 1) * hr, :].astype(F32)
            last(p, tot)

    chunk = part.shape[0] // nz
    hr = chunk // SUM_PIECES
    loads[0].wait()
    part[...] = dot(att[...], wown[...])
    remote(w.at[:, other_half], wsib, ws.at[0], wr.at[0], sib).wait_recv()
    swap.wait_recv()
    part[...] += dot(pair[...], wsib[...])

    def own_b(zz, p):
        return part[pl.ds(pl.multiple_of(zz * chunk + p * hr, hr), hr), :]

    crow = chunk // 2

    def last_b(p, tot):
        for i in range(max(1, hr // crow)):
            r = p * hr + i * crow if hr >= crow else p * hr
            cnt = min(hr, crow)
            core = r // crow
            at = r % crow
            piece = tot[i * crow : i * crow + cnt] if hr >= crow else tot

            @pl.when(c == core)
            def _():
                ybuf[c, at : at + cnt, :] = piece

            @pl.when(c != core)
            def _():
                xbuf[at : at + cnt, :] = piece

    ring_sum(own_b, sbb, rbb, bs, br, SUM_PIECES, hr, last_b)
    trade = remote(xbuf, ybuf.at[c], es, er, sib)
    start(trade)
    remote(xbuf, ybuf.at[1 - c], es, er, sib).wait_recv()
    lo = res[:, :half].astype(F32) + ybuf[0]
    hi = res[:, half:].astype(F32) + ybuf[1]
    mlo, mhi = lo.astype(BF), hi.astype(BF)
    mixed[:, :half] = mlo
    mixed[:, half:] = mhi
    lo, hi = mlo.astype(F32), mhi.astype(F32)
    mean = (
        jnp.sum(lo * lo, axis=1, keepdims=True) + jnp.sum(hi * hi, axis=1, keepdims=True)
    ) / (2 * half)
    scale = lax.rsqrt(mean + 1e-06)
    nlo = (lo * scale * gain[:, :half]).astype(BF)
    nhi = (hi * scale * gain[:, half:]).astype(BF)

    tok = res.shape[0]
    here = iota((tok, KB), 1) == (z * 2 + c) * tok + iota((tok, KB), 0)
    chosen = [
        jnp.sum(jnp.where(here, ids[i : i + 1, :], 0), axis=1, keepdims=True) for i in range(2)
    ]
    eye16 = iota((tok, tok), 0) == iota((tok, tok), 1)
    trow = [
        jnp.sum(jnp.where(eye16, chosen[i], 0), axis=0, keepdims=True)
        for i in range(2)
    ]
    slot = iota((2 * n, tok), 0)
    expert_of = lax.div(slot, 2)
    named = ((trow[0] == expert_of) | (trow[1] == expert_of)).astype(F32)
    earlier = (iota((tok, tok), 0) < iota((tok, tok), 1)).astype(BF)
    rank = dot(named.astype(BF), earlier)
    odd = lax.rem(slot, 2).astype(F32)
    pick = jnp.where(rank == odd, named, 0.0).astype(BF)
    slo = dot(pick, nlo).astype(BF)
    shi = dot(pick, nhi).astype(BF)
    for e in range(n):
        sent[e, :, :half] = slo[2 * e : 2 * e + 2, :]
        sent[e, :, half:] = shi[2 * e : 2 * e + 2, :]

    for d, (ty, tx, t) in enumerate(others):
        start(remote(sent.at[t], inb.at[me], is_.at[d], ir.at[me], (ty, tx, z, c)))
    inb[me] = sent[me]

    normed = jnp.concatenate([nlo, nhi], axis=1)
    loads[4].wait()
    loads[5].wait()
    glog = dot_t(normed, grw[...])
    elog = dot_t(normed, exw[...])
    margin = glog[:, 0:1] - glog[:, 1:2]
    own_margin = jnp.where(chosen[0] < n // GROUPS, margin, -margin)
    share = jax.nn.sigmoid(own_margin)
    eid = iota((tok, n), 1)
    picked = [
        jnp.sum(jnp.where(chosen[i] == eid, elog, 0.0), axis=1, keepdims=True)
        for i in range(2)
    ]
    route = [share * jax.nn.sigmoid(picked[i] - picked[1 - i]) for i in range(2)]
    slot_c = iota((tok, 2 * n), 1)
    exp_c = lax.div(slot_c, 2)
    is_k = [chosen[i] == exp_c for i in range(2)]
    named_c = (is_k[0] | is_k[1]).astype(BF)
    before = (iota((tok, tok), 1) < iota((tok, tok), 0)).astype(BF)
    rank_c = dot(before, named_c)
    odd_c = lax.rem(slot_c, 2).astype(F32)
    take = [
        jnp.where(is_k[i] & (rank_c == odd_c), 1.0, 0.0).astype(BF) for i in range(2)
    ]

    for ty, tx, t in others:
        remote(sent.at[t], inb.at[t], is_.at[0], ir.at[t], sib).wait_recv()
    mine = z * 2 + c
    for e in range(n):
        rows[mine, 2 * e : 2 * e + 2, :] = inb[e]

    per = rows.shape[1]
    hb = per // ROW_PIECES

    def piece(b, p):
        return rows.at[b, pl.ds(p * hb, hb), :]

    def from_chip(d, h):
        return lax.rem(z + nz - h, nz) if d == 0 else lax.rem(z + h, nz)

    def hop(d, h, p):
        b = from_chip(d, h - 1) * 2 + c
        return remote(
            piece(b, p), piece(b, p), gs.at[d, h, p], gr.at[d, h, p], right if d == 0 else left
        )

    def got_hop(d, h, p):
        b = from_chip(d, h) * 2 + c
        return remote(piece(b, p), piece(b, p), gs.at[d, h, p], gr.at[d, h, p], sib)

    def cross(d, h, p, core):
        b = from_chip(d, h) * 2 + core
        return remote(piece(b, p), piece(b, p), cs.at[d, h, p], cr.at[d, h, p], sib)

    def pieces(d, h):
        if h < far:
            return list(range(ROW_PIECES))
        hp = ROW_PIECES // 2
        return list(range(hp)) if d == 0 else list(range(hp, ROW_PIECES))

    def order(d):
        hp = ROW_PIECES // 2
        a = list(range(hp))
        b = list(range(hp, ROW_PIECES))
        return a + b if d == 0 else b + a

    for i in range(ROW_PIECES):
        for d in (0, 1):
            start(hop(d, 1, order(d)[i]))
    for p in range(ROW_PIECES):
        start(cross(0, 0, p, c))

    def blocks_of(h):
        if h == 0:
            return [(z * 2 + i, i) for i in (0, 1)]
        lo_ = from_chip(0, h)
        hi_ = from_chip(1, h)
        if h == far:
            return [(lo_ * 2 + i, 4 * h - 2 + i) for i in (0, 1)]
        return [(lo_ * 2 + i, 4 * h - 2 + i) for i in (0, 1)] + [
            (hi_ * 2 + i, 4 * h + i) for i in (0, 1)
        ]

    def hswap(b, i):
        return remote(hid.at[0, b], hid.at[1, b], hs_.at[i], hr_.at[i], sib)

    def run(h):
        for d in (0, 1):
            if h == 0 and d == 1:
                continue
            for p in pieces(d, h):
                cross(d, h, p, 1 - c).wait_recv()
        bl = blocks_of(h)
        xin = jnp.concatenate([rows[b] for b, i in bl], axis=0)
        g = dot(xin, gw[...])
        u = dot(xin, uw[...])
        hv = (g * jax.nn.sigmoid(g) * u).astype(BF)
        for j, (b, i) in enumerate(bl):
            hid[0, b] = hv[j * per : (j + 1) * per]
            start(hswap(b, i))

    def finish(h):
        bl = blocks_of(h)
        for b, i in bl:
            hswap(b, i).wait_recv()
        h0 = jnp.concatenate([hid[0, b] for b, i in bl], axis=0)
        h1 = jnp.concatenate([hid[1, b] for b, i in bl], axis=0)
        val = dot(h0, dw[...]) + dot(h1, dsib[...])
        for j, (b, i) in enumerate(bl):
            partc[b] = val[j * per : (j + 1) * per]

    loads[1].wait()
    loads[2].wait()
    for h in range(1, far + 1):
        for i in range(ROW_PIECES):
            for d in (0, 1):
                p = order(d)[i]
                if p not in pieces(d, h):
                    continue
                got_hop(d, h, p).wait_recv()
                if h + 1 <= far and p in pieces(d, h + 1):
                    start(hop(d, h + 1, p))
                start(cross(d, h, p, c))
            if i == 0:
                run(h - 1)
                if h == 1:
                    loads[3].wait()
                    remote(down.at[:, other_half], dsib, ws.at[1], wr.at[1], sib).wait_recv()
            if i == 1:
                finish(h - 1)
    run(far)
    finish(far)

    chunk_c = 2 * per
    hc = chunk_c // BACK_PIECES

    def own_c(zz, p):
        b = zz * 2 + (p * hc) // per
        return partc[b, (p * hc) % per : (p * hc) % per + hc, :]

    def last_c(p, tot):
        core = (p * hc) // per
        e0 = ((p * hc) % per) // 2
        tb = tot.astype(BF)
        for e in range(hc // 2):
            t = e0 + e
            fin[core, t] = tb[2 * e : 2 * e + 2, :]
            ty, tx = t // nx, t % nx

            @pl.when(me != t)
            def _(t=t, ty=ty, tx=tx):
                remote(
                    fin.at[core, t], ret.at[c, me], fs.at[core, t], fr.at[c, me], (ty, tx, z, core)
                ).start()

            @pl.when((me == t) & (c != core))
            def _(t=t):
                remote(
                    fin.at[core, t], ret.at[c, me], fs.at[core, t], fr.at[c, me], sib
                ).start()

    ring_sum(own_c, sbc, rbc, ss, rs, BACK_PIECES, hc, last_c)
    ret[c, me] = fin[c, me]
    for i in (0, 1):
        for t in range(n):

            @pl.when((me != t) | (c != i))
            def _(t=t, i=i):
                remote(fin.at[0, t], ret.at[i, t], fs.at[0, t], fr.at[i, t], sib).wait_recv()

            back[2 * t : 2 * t + 2, i * half : (i + 1) * half] = ret[i, t]
    for i in range(2):
        cols = slice(i * half, (i + 1) * half)
        bk = back[:, cols]
        mix = route[0] * dot(take[0], bk) + route[1] * dot(take[1], bk)
        out[:, cols] = mixed[:, cols].astype(F32) + mix

    for cond, copies in plan:

        @pl.when(cond)
        def _(copies=copies):
            for a in copies:
                a.wait_send()

    for core in (0, 1):
        for t in range(n):

            @pl.when((me != t) | (c != core))
            def _(t=t, core=core):
                remote(
                    fin.at[core, t], ret.at[c, me], fs.at[core, t], fr.at[c, me], sib
                ).wait_send()

    for a in sends:
        a.wait_send()


def per_device(
    residual_in, queries, keys, values, break_offset, doc_ids, out_weight, norm_gain,
    group_router, expert_router, expert_ids, gate_weight, up_weight, down_weight,
):
    ny, nx, nz = lax.axis_size("y"), lax.axis_size("x"), lax.axis_size("z")
    n = ny * nx
    rows, att = queries.shape
    tok, width = residual_in.shape
    half = width // 2
    heads = break_offset.shape[1]
    gate, up, down = gate_weight[0], up_weight[0], down_weight[0]
    units = gate.shape[1]
    per = 2 * n
    far = nz // 2
    sends = (nx - 1) + (ny - 1) + (nx - 1) * (ny - 1)
    dma = pltpu.SemaphoreType.DMA
    vm = pltpu.VMEM
    scratch = [
        vm((tok, width), BF), vm((rows, att), BF), vm((rows, att), BF), vm((rows, att), BF),
        vm((heads, rows), BF), vm((1, rows), jnp.int32), vm((1, width), F32),
        vm((2, rows), jnp.int32),
        vm((n, rows, att), BF), vm((n, rows, att), BF), vm((n, 16, rows), BF), vm((16, rows), BF),
        vm((KB, KB), BF), vm((rows, att), BF), vm((rows, 1), F32), vm((rows, att), F32),
        vm((heads, rows, 1), F32),
        vm((att, half), BF), vm((att, half), BF), vm((rows, att), BF), vm((rows, att), BF),
        vm((rows, half), F32),
        vm((2, far, rows // nz, half), BF), vm((2, far, rows // nz, half), BF),
        vm((tok, half), F32), vm((2, tok, half), F32), vm((tok, width), BF),
        vm((n, 2, width), BF), vm((n, 2, width), BF), vm((2 * nz, per, width), BF),
        vm((width, units), BF), vm((width, units), BF), vm((units, half), BF),
        vm((units, half), BF),
        vm((2, 2 * nz, per, units), BF), vm((2 * nz, per, half), F32),
        vm((2, far, 2 * per, half), BF), vm((2, far, 2 * per, half), BF),
        vm((2, n, 2, half), BF), vm((2, n, 2, half), BF), vm((per, width), BF),
        vm((GROUPS, width), BF), vm((n, width), BF),
        dma((14,)),
        dma((sends,)), dma((n,)), dma((sends,)), dma((n,)), dma((sends,)), dma((n,)),
        dma((2,)), dma((2,)), dma, dma,
        dma((2, far, SUM_PIECES)), dma((2, far, SUM_PIECES)), dma, dma,
        dma((n - 1,)), dma((n,)),
        dma((2, far + 1, ROW_PIECES)), dma((2, far + 1, ROW_PIECES)),
        dma((2, far + 1, ROW_PIECES)), dma((2, far + 1, ROW_PIECES)),
        dma((2 * nz,)), dma((2 * nz,)),
        dma((2, far, BACK_PIECES)), dma((2, far, BACK_PIECES)),
        dma((2, n)), dma((2, n)),
    ]
    summed = pl.pallas_call(
        functools.partial(layer_kernel, (ny, nx, nz)),
        out_shape=jax.ShapeDtypeStruct(residual_in.shape, F32),
        in_specs=[ANY] * 14,
        out_specs=VM,
        scratch_shapes=scratch,
        compiler_params=pltpu.CompilerParams(
            collective_id=1, has_side_effects=True, vmem_limit_bytes=LIMIT
        ),
        name="layer",
    )(
        residual_in, queries, keys, values, break_offset.T, doc_ids[None, :], out_weight,
        norm_gain[None, :], group_router.T, expert_router.T, expert_ids.T, gate, up, down,
    )
    return summed.astype(BF)


def solution(mesh):
    n = mesh.shape["sp"]
    side = round(n**0.5)
    finer = Mesh(mesh.devices.reshape(side, n // side, mesh.shape["tp"] // 2, 2), AXES)
    in_specs = (
        P(SP + TP, None),
        P(SP, TP),
        P(SP, TP),
        P(SP, TP),
        P(SP, TP),
        P(SP),
        P(TP, None),
        P(),
        P(),
        P(),
        P(SP, None),
        P(SP, None, TP),
        P(SP, None, TP),
        P(SP, TP, None),
    )
    return jax.shard_map(
        per_device, mesh=finer, in_specs=in_specs, out_specs=P(SP + TP, None), check_vma=False
    )
```

```python
import functools

import jax
import jax.numpy as jnp
from jax import lax
from jax.experimental import pallas as pl
from jax.experimental.pallas import tpu as pltpu
from jax.sharding import Mesh
from jax.sharding import PartitionSpec as P

HEAD_DIM = 64
GROUPS = 2
DOC_MOST = 2560
KB = 256
BAND = DOC_MOST // KB
NEG = -1e30
SUM_PIECES = 2
ROW_PIECES = 4
BACK_PIECES = 4
NEAR = (0, 1, 3, 2)
MESH = pl.DeviceIdType.MESH
AXES = ("y", "x", "z", "c")
SP = ("y", "x")
TP = ("z", "c")
VM = pl.BlockSpec(memory_space=pltpu.VMEM)
ANY = pl.BlockSpec(memory_space=pl.ANY)
BF = jnp.bfloat16
F32 = jnp.float32
LIMIT = 60 * 1024 * 1024


def dot(a, b):
    return jnp.dot(a, b, preferred_element_type=F32)


def dot_t(a, b):
    return lax.dot_general(a, b, (((1,), (1,)), ((), ())), preferred_element_type=F32)


def iota(shape, axis):
    return lax.broadcasted_iota(jnp.int32, shape, axis)


def remote(src, dst, ss, rs, to):
    return pltpu.make_async_remote_copy(
        src_ref=src, dst_ref=dst, send_sem=ss, recv_sem=rs, device_id=to, device_id_type=MESH
    )


def attend_block(diag, q, kb, vb, ab, qd, part_out, part_go, later):
    heads = range(q.shape[1] // HEAD_DIM)
    rows = q.shape[0]
    cols = [slice(h * HEAD_DIM, (h + 1) * HEAD_DIM) for h in heads]
    scores = [dot_t(q[:, cols[h]], kb[:, cols[h]]) for h in heads]
    live = ab[len(heads) : len(heads) + 1, :].astype(F32) == qd[...]
    if diag:
        live = live & (iota((rows, KB), 1) < iota((rows, KB), 0))
    log_w, total = [], []
    for h in heads:
        s = jnp.where(live, scores[h] + ab[h : h + 1, :].astype(F32), NEG)
        go = jnp.maximum(s, 0.0) + jnp.log(1.0 + jnp.exp(-jnp.abs(s)))
        hi = go.astype(BF)
        lo = (go - hi.astype(F32)).astype(BF)
        total.append(jnp.sum(go, axis=1, keepdims=True))
        log_w.append((s - go, dot(hi, later[...]) + dot(lo, later[...])))
    for h in heads:
        o = dot(jnp.exp(log_w[h][0] - log_w[h][1]).astype(BF), vb[:, cols[h]])
        part_out[:, cols[h]] = o
        part_go[h] = total[h]


def layer_kernel(
    dims,
    res_, q_, k_, v_, off_, doc_, w, gain_, grp, exr, ids_, gate, up, down,
    out,
    res, q, k, v, off, doc, gain, ids,
    kall, vall, aall, auxo, later, qs, qd, acc, st, run, tot_out,
    wown, wsib, att, pair, part, sbb, rbb, xbuf, ybuf, mixed,
    sent, inb, rows, gw, uw, dw, dsib, hid, partc, sbc, rbc, fin, ret, back, grw, exw,
    lsem, ks, kr, vs, vr, as_, ar, ws, wr, ds, dr, bs, br, es, er,
    is_, ir, gs, gr, cs, cr, hs_, hr_, ss, rs, fs, fr,
):
    ny, nx, nz = dims
    y, x, z, c = (lax.axis_index(a) for a in AXES)
    me = y * nx + x
    n = ny * nx
    sib = (y, x, z, 1 - c)
    right = (y, x, lax.rem(z + 1, nz), c)
    left = (y, x, lax.rem(z + nz - 1, nz), c)
    half = wown.shape[1]
    heads = off.shape[0]
    own_half = pl.ds(pl.multiple_of(c * half, half), half)
    other_half = pl.ds(pl.multiple_of((1 - c) * half, half), half)
    far = nz // 2
    sends = []

    def start(q_):
        q_.start()
        sends.append(q_)

    others = []
    for dy in NEAR:
        for dx in range(nx):
            if dy or dx:
                ty, tx = lax.rem(y + dy, ny), lax.rem(x + dx, nx)
                others.append((ty, tx, ty * nx + tx))
    peers = [(ty, tx, z, c) for ty, tx, t in others]
    peers += [(ty, tx, z, 1 - c) for ty, tx, t in others]
    peers += [right, left, sib]
    bar = pltpu.get_barrier_semaphore()
    for p in peers:
        pl.semaphore_signal(bar, inc=1, device_id=p, device_id_type=MESH)
    small = [
        pltpu.make_async_copy(a, b, lsem.at[6 + i])
        for i, (a, b) in enumerate(
            [(off_, off), (doc_, doc), (k_, k), (v_, v), (q_, q), (ids_, ids), (gain_, gain), (res_, res)]
        )
    ]
    loads = [
        pltpu.make_async_copy(w.at[:, own_half], wown, lsem.at[0]),
        pltpu.make_async_copy(gate, gw, lsem.at[1]),
        pltpu.make_async_copy(up, uw, lsem.at[2]),
        pltpu.make_async_copy(down.at[:, own_half], dw, lsem.at[3]),
        pltpu.make_async_copy(grp, grw, lsem.at[4]),
        pltpu.make_async_copy(exr, exw, lsem.at[5]),
    ]
    for a in small + loads:
        a.start()

    later[...] = (iota((KB, KB), 0) > iota((KB, KB), 1)).astype(BF)
    for a in small:
        a.wait()
    docf = doc[...].astype(F32)
    eye = iota((KB, KB), 0) == iota((KB, KB), 1)
    qd[...] = jnp.sum(jnp.where(eye, docf, 0.0), axis=1, keepdims=True)
    pad = jnp.zeros((auxo.shape[0] - heads - 1, KB), F32)
    auxo[...] = jnp.concatenate([off[...].astype(F32), docf, pad], axis=0).astype(BF)
    qs[...] = q[...] * BF(HEAD_DIM**-0.5)
    pl.semaphore_wait(bar, len(peers))

    xs = [lax.rem(x + d, nx) for d in range(1, nx)]
    ys = [lax.rem(y + d, ny) for d in range(1, ny)]
    xb = [lax.rem(x + nx - d, nx) for d in range(1, nx)]
    yb = [lax.rem(y + ny - d, ny) for d in range(1, ny)]

    def used(b, j):
        return (j > b) & (j - b <= BAND)

    def k_first(src, dst):
        return (dst > src) | (y < ny - 1)

    def v_first(dst, src, col):
        return (dst > src) & (nx * (dst - src) - col <= BAND)

    def kcopy(b, src, asrc, i, to):
        return (
            remote(src, kall.at[b], ks.at[i], kr.at[b], to),
            remote(asrc, aall.at[b], as_.at[i], ar.at[b], to),
        )

    def vcopy(b, src, i, to):
        return (remote(src, vall.at[b], vs.at[i], vr.at[b], to),)

    plan = []

    def send(cond, copies):
        plan.append((cond, copies))

        @pl.when(cond)
        def _():
            for a in copies:
                a.start()

    def arrive(cond, copies):
        @pl.when(cond)
        def _():
            for a in copies:
                a.wait_recv()

    nk = nv = 0
    for a in xs:
        send(k_first(x, a), kcopy(me, k, auxo, nk, (y, a, z, c)))
        nk += 1
    for a in ys:
        send(v_first(a, y, x), vcopy(me, v, nv, (a, x, z, c)))
        nv += 1
    for a in ys:
        send(used(me, a * nx + x), kcopy(me, k, auxo, nk, (a, x, z, c)))
        nk += 1
    for a in xs:
        send(used(me, y * nx + a), vcopy(me, v, nv, (y, a, z, c)))
        nv += 1
    start(remote(w.at[:, other_half], wsib, ws.at[0], wr.at[0], sib))
    start(remote(down.at[:, other_half], dsib, ws.at[1], wr.at[1], sib))

    attend_block(True, qs, k, v, auxo, qd, acc.at[me], st.at[me], later)

    firsts = []
    for i in range(max(nx, ny) - 1):
        if i < nx - 1:
            b = y * nx + xb[i]
            got = k_first(xb[i], x)
            arrive(got, kcopy(b, k, auxo, 0, sib))
            for a in ys:
                send(got & used(b, a * nx + x), kcopy(b, kall.at[b], aall.at[b], nk, (a, x, z, c)))
                nk += 1
        if i < ny - 1:
            b = yb[i] * nx + x
            got = v_first(y, yb[i], x)
            arrive(got, vcopy(b, v, 0, sib))
            for a in xs:
                send(got & used(b, y * nx + a), vcopy(b, vall.at[b], nv, (y, a, z, c)))
                nv += 1
    del firsts

    def step(b):
        by = lax.div(b, nx)
        bx = lax.rem(b, nx)

        @pl.when(by != y)
        def _():
            for a in kcopy(b, k, auxo, 0, sib):
                a.wait_recv()

        @pl.when(bx != x)
        def _():
            for a in vcopy(b, v, 0, sib):
                a.wait_recv()

        attend_block(
            False, qs, kall.at[b], vall.at[b], aall.at[b], qd, acc.at[b], st.at[b], later
        )

    def walk(i, carry):
        b = (y - lax.rem(i, ny)) * nx + lax.rem(x + nx - lax.div(i, ny), nx)

        @pl.when((b >= 0) & used(b, me))
        def _():
            step(b)

        return carry

    lax.fori_loop(1, n, walk, 0)
    run[...] = st[me]
    tot_out[...] = acc[me]

    def gather(t, carry):
        b = me - t
        for h in range(heads):
            hs = slice(h * HEAD_DIM, (h + 1) * HEAD_DIM)
            before = run[h]
            tot_out[:, hs] = tot_out[:, hs] + jnp.exp(-before) * acc[b, :, hs]
            run[h] = before + st[b, h]
        return carry

    lax.fori_loop(1, jnp.minimum(me, BAND) + 1, gather, 0)
    att[...] = tot_out[...].astype(BF)
    swap = remote(att, pair, ds, dr, sib)
    start(swap)

    def ring_sum(own, sbuf, rbuf, s_sem, r_sem, np_, hr, last):
        def move(d, s, p):
            ref = (d, s, pl.ds(p * hr, hr))
            return remote(
                sbuf.at[ref], rbuf.at[ref], s_sem.at[d, s, p], r_sem.at[d, s, p],
                right if d == 0 else left,
            )

        def half_of(d):
            return range(np_ // 2) if d == 0 else range(np_ // 2, np_)

        for s in range(far):
            for i in range(np_ // 2 if s == 0 else np_):
                for d in range(2):
                    order = list(half_of(d)) + ([] if s == 0 else list(half_of(1 - d)))
                    p = order[i]
                    dist = far - s
                    zz = lax.rem(z + dist, nz) if d == 0 else lax.rem(z + nz - dist, nz)
                    val = own(zz, p)
                    if s > 1 or (s == 1 and p in half_of(d)):
                        move(d, s - 1, p).wait_recv()
                        val = val + rbuf[d, s - 1, p * hr : (p + 1) * hr, :].astype(F32)
                    sbuf[d, s, p * hr : (p + 1) * hr, :] = val.astype(BF)
                    start(move(d, s, p))
        for i in range(np_):
            p = i
            for d in range(2):
                move(d, far - 1, p).wait_recv()
            tot = own(z, p)
            for d in range(2):
                tot = tot + rbuf[d, far - 1, p * hr : (p + 1) * hr, :].astype(F32)
            last(p, tot)

    chunk = part.shape[0] // nz
    hr = chunk // SUM_PIECES
    loads[0].wait()
    part[...] = dot(att[...], wown[...])
    remote(w.at[:, other_half], wsib, ws.at[0], wr.at[0], sib).wait_recv()
    swap.wait_recv()
    part[...] += dot(pair[...], wsib[...])

    def own_b(zz, p):
        return part[pl.ds(pl.multiple_of(zz * chunk + p * hr, hr), hr), :]

    crow = chunk // 2

    def last_b(p, tot):
        for i in range(max(1, hr // crow)):
            r = p * hr + i * crow if hr >= crow else p * hr
            cnt = min(hr, crow)
            core = r // crow
            at = r % crow
            piece = tot[i * crow : i * crow + cnt] if hr >= crow else tot

            @pl.when(c == core)
            def _():
                ybuf[c, at : at + cnt, :] = piece

            @pl.when(c != core)
            def _():
                xbuf[at : at + cnt, :] = piece

    ring_sum(own_b, sbb, rbb, bs, br, SUM_PIECES, hr, last_b)
    trade = remote(xbuf, ybuf.at[c], es, er, sib)
    start(trade)
    remote(xbuf, ybuf.at[1 - c], es, er, sib).wait_recv()
    lo = res[:, :half].astype(F32) + ybuf[0]
    hi = res[:, half:].astype(F32) + ybuf[1]
    mlo, mhi = lo.astype(BF), hi.astype(BF)
    mixed[:, :half] = mlo
    mixed[:, half:] = mhi
    lo, hi = mlo.astype(F32), mhi.astype(F32)
    mean = (
        jnp.sum(lo * lo, axis=1, keepdims=True) + jnp.sum(hi * hi, axis=1, keepdims=True)
    ) / (2 * half)
    scale = lax.rsqrt(mean + 1e-06)
    nlo = (lo * scale * gain[:, :half]).astype(BF)
    nhi = (hi * scale * gain[:, half:]).astype(BF)

    tok = res.shape[0]
    here = iota((tok, KB), 1) == (z * 2 + c) * tok + iota((tok, KB), 0)
    chosen = [
        jnp.sum(jnp.where(here, ids[i : i + 1, :], 0), axis=1, keepdims=True) for i in range(2)
    ]
    eye16 = iota((tok, tok), 0) == iota((tok, tok), 1)
    trow = [
        jnp.sum(jnp.where(eye16, chosen[i], 0), axis=0, keepdims=True)
        for i in range(2)
    ]
    slot = iota((2 * n, tok), 0)
    expert_of = lax.div(slot, 2)
    named = ((trow[0] == expert_of) | (trow[1] == expert_of)).astype(F32)
    earlier = (iota((tok, tok), 0) < iota((tok, tok), 1)).astype(BF)
    rank = dot(named.astype(BF), earlier)
    odd = lax.rem(slot, 2).astype(F32)
    pick = jnp.where(rank == odd, named, 0.0).astype(BF)
    slo = dot(pick, nlo).astype(BF)
    shi = dot(pick, nhi).astype(BF)
    for e in range(n):
        sent[e, :, :half] = slo[2 * e : 2 * e + 2, :]
        sent[e, :, half:] = shi[2 * e : 2 * e + 2, :]

    for d, (ty, tx, t) in enumerate(others):
        start(remote(sent.at[t], inb.at[me], is_.at[d], ir.at[me], (ty, tx, z, c)))
    inb[me] = sent[me]

    normed = jnp.concatenate([nlo, nhi], axis=1)
    loads[4].wait()
    loads[5].wait()
    glog = dot_t(normed, grw[...])
    elog = dot_t(normed, exw[...])
    margin = glog[:, 0:1] - glog[:, 1:2]
    own_margin = jnp.where(chosen[0] < n // GROUPS, margin, -margin)
    share = jax.nn.sigmoid(own_margin)
    eid = iota((tok, n), 1)
    picked = [
        jnp.sum(jnp.where(chosen[i] == eid, elog, 0.0), axis=1, keepdims=True)
        for i in range(2)
    ]
    route = [share * jax.nn.sigmoid(picked[i] - picked[1 - i]) for i in range(2)]
    slot_c = iota((tok, 2 * n), 1)
    exp_c = lax.div(slot_c, 2)
    is_k = [chosen[i] == exp_c for i in range(2)]
    named_c = (is_k[0] | is_k[1]).astype(BF)
    before = (iota((tok, tok), 1) < iota((tok, tok), 0)).astype(BF)
    rank_c = dot(before, named_c)
    odd_c = lax.rem(slot_c, 2).astype(F32)
    take = [
        jnp.where(is_k[i] & (rank_c == odd_c), 1.0, 0.0).astype(BF) for i in range(2)
    ]

    mine = z * 2 + c

    per = rows.shape[1]
    hb = per // ROW_PIECES

    def spot(p):
        return pl.multiple_of(lax.rem(y + NEAR[p], ny) * hb, hb)

    def piece(b, p):
        return rows.at[b, pl.ds(spot(p), hb), :]

    def from_chip(d, h):
        return lax.rem(z + nz - h, nz) if d == 0 else lax.rem(z + h, nz)

    def hop(d, h, p):
        b = from_chip(d, h - 1) * 2 + c
        return remote(
            piece(b, p), piece(b, p), gs.at[d, h, p], gr.at[d, h, p], right if d == 0 else left
        )

    def got_hop(d, h, p):
        b = from_chip(d, h) * 2 + c
        return remote(piece(b, p), piece(b, p), gs.at[d, h, p], gr.at[d, h, p], sib)

    def cross(d, h, p, core):
        b = from_chip(d, h) * 2 + core
        return remote(piece(b, p), piece(b, p), cs.at[d, h, p], cr.at[d, h, p], sib)

    def pieces(d, h):
        if h < far:
            return list(range(ROW_PIECES))
        hp = ROW_PIECES // 2
        return list(range(hp)) if d == 0 else list(range(hp, ROW_PIECES))

    def order(d):
        return (0, 1, 2, 3) if d == 0 else (0, 2, 3, 1)

    def out_pieces(k):
        return [(0, k)] + {0: [(1, 0)], 1: [], 2: [(1, 2)], 3: [(1, 3), (1, 1)]}[k]

    for p in range(ROW_PIECES):
        ty = lax.rem(y + NEAR[p], ny)
        for dx in range(nx):
            if NEAR[p] or dx:
                t = ty * nx + lax.rem(x + dx, nx)
                remote(sent.at[t], inb.at[t], is_.at[0], ir.at[t], sib).wait_recv()
        rows[mine, pl.ds(spot(p), hb), :] = jnp.concatenate(
            [inb[ty * nx + q_] for q_ in range(nx)], axis=0
        )
        for d, k_ in out_pieces(p):
            start(hop(d, 1, k_))
        start(cross(0, 0, p, c))

    def blocks_of(h):
        if h == 0:
            return [(z * 2 + i, i) for i in (0, 1)]
        lo_ = from_chip(0, h)
        hi_ = from_chip(1, h)
        if h == far:
            return [(lo_ * 2 + i, 4 * h - 2 + i) for i in (0, 1)]
        return [(lo_ * 2 + i, 4 * h - 2 + i) for i in (0, 1)] + [
            (hi_ * 2 + i, 4 * h + i) for i in (0, 1)
        ]

    def hswap(b, i):
        return remote(hid.at[0, b], hid.at[1, b], hs_.at[i], hr_.at[i], sib)

    def run(h):
        for d in (0, 1):
            if h == 0 and d == 1:
                continue
            for p in pieces(d, h):
                cross(d, h, p, 1 - c).wait_recv()
        bl = blocks_of(h)
        xin = jnp.concatenate([rows[b] for b, i in bl], axis=0)
        g = dot(xin, gw[...])
        u = dot(xin, uw[...])
        hv = (g * jax.nn.sigmoid(g) * u).astype(BF)
        for j, (b, i) in enumerate(bl):
            hid[0, b] = hv[j * per : (j + 1) * per]
            start(hswap(b, i))

    def finish(h):
        bl = blocks_of(h)
        for b, i in bl:
            hswap(b, i).wait_recv()
        h0 = jnp.concatenate([hid[0, b] for b, i in bl], axis=0)
        h1 = jnp.concatenate([hid[1, b] for b, i in bl], axis=0)
        val = dot(h0, dw[...]) + dot(h1, dsib[...])
        for j, (b, i) in enumerate(bl):
            partc[b] = val[j * per : (j + 1) * per]

    loads[1].wait()
    loads[2].wait()
    for h in range(1, far + 1):
        for i in range(ROW_PIECES):
            for d in (0, 1):
                p = order(d)[i]
                if p not in pieces(d, h):
                    continue
                got_hop(d, h, p).wait_recv()
                if h + 1 <= far and p in pieces(d, h + 1):
                    start(hop(d, h + 1, p))
                start(cross(d, h, p, c))
            if i == 0:
                run(h - 1)
                if h == 1:
                    loads[3].wait()
                    remote(down.at[:, other_half], dsib, ws.at[1], wr.at[1], sib).wait_recv()
            if i == 1:
                finish(h - 1)
    run(far)
    finish(far)

    chunk_c = 2 * per
    hc = chunk_c // BACK_PIECES

    def own_c(zz, p):
        b = zz * 2 + (p * hc) // per
        return partc[b, (p * hc) % per : (p * hc) % per + hc, :]

    def last_c(p, tot):
        core = (p * hc) // per
        e0 = ((p * hc) % per) // 2
        tb = tot.astype(BF)
        for e in range(hc // 2):
            t = e0 + e
            fin[core, t] = tb[2 * e : 2 * e + 2, :]
            ty, tx = t // nx, t % nx

            @pl.when(me != t)
            def _(t=t, ty=ty, tx=tx):
                remote(
                    fin.at[core, t], ret.at[c, me], fs.at[core, t], fr.at[c, me], (ty, tx, z, core)
                ).start()

            @pl.when((me == t) & (c != core))
            def _(t=t):
                remote(
                    fin.at[core, t], ret.at[c, me], fs.at[core, t], fr.at[c, me], sib
                ).start()

    ring_sum(own_c, sbc, rbc, ss, rs, BACK_PIECES, hc, last_c)
    ret[c, me] = fin[c, me]
    for i in (0, 1):
        for t in range(n):

            @pl.when((me != t) | (c != i))
            def _(t=t, i=i):
                remote(fin.at[0, t], ret.at[i, t], fs.at[0, t], fr.at[i, t], sib).wait_recv()

            back[2 * t : 2 * t + 2, i * half : (i + 1) * half] = ret[i, t]
    for i in range(2):
        cols = slice(i * half, (i + 1) * half)
        bk = back[:, cols]
        mix = route[0] * dot(take[0], bk) + route[1] * dot(take[1], bk)
        out[:, cols] = mixed[:, cols].astype(F32) + mix

    for cond, copies in plan:

        @pl.when(cond)
        def _(copies=copies):
            for a in copies:
                a.wait_send()

    for core in (0, 1):
        for t in range(n):

            @pl.when((me != t) | (c != core))
            def _(t=t, core=core):
                remote(
                    fin.at[core, t], ret.at[c, me], fs.at[core, t], fr.at[c, me], sib
                ).wait_send()

    for a in sends:
        a.wait_send()


def per_device(
    residual_in, queries, keys, values, break_offset, doc_ids, out_weight, norm_gain,
    group_router, expert_router, expert_ids, gate_weight, up_weight, down_weight,
):
    ny, nx, nz = lax.axis_size("y"), lax.axis_size("x"), lax.axis_size("z")
    n = ny * nx
    rows, att = queries.shape
    tok, width = residual_in.shape
    half = width // 2
    heads = break_offset.shape[1]
    gate, up, down = gate_weight[0], up_weight[0], down_weight[0]
    units = gate.shape[1]
    per = 2 * n
    far = nz // 2
    sends = (nx - 1) + (ny - 1) + (nx - 1) * (ny - 1)
    dma = pltpu.SemaphoreType.DMA
    vm = pltpu.VMEM
    scratch = [
        vm((tok, width), BF), vm((rows, att), BF), vm((rows, att), BF), vm((rows, att), BF),
        vm((heads, rows), BF), vm((1, rows), jnp.int32), vm((1, width), F32),
        vm((2, rows), jnp.int32),
        vm((n, rows, att), BF), vm((n, rows, att), BF), vm((n, 16, rows), BF), vm((16, rows), BF),
        vm((KB, KB), BF), vm((rows, att), BF), vm((rows, 1), F32), vm((n, rows, att), F32),
        vm((n, heads, rows, 1), F32), vm((heads, rows, 1), F32), vm((rows, att), F32),
        vm((att, half), BF), vm((att, half), BF), vm((rows, att), BF), vm((rows, att), BF),
        vm((rows, half), F32),
        vm((2, far, rows // nz, half), BF), vm((2, far, rows // nz, half), BF),
        vm((tok, half), F32), vm((2, tok, half), F32), vm((tok, width), BF),
        vm((n, 2, width), BF), vm((n, 2, width), BF), vm((2 * nz, per, width), BF),
        vm((width, units), BF), vm((width, units), BF), vm((units, half), BF),
        vm((units, half), BF),
        vm((2, 2 * nz, per, units), BF), vm((2 * nz, per, half), F32),
        vm((2, far, 2 * per, half), BF), vm((2, far, 2 * per, half), BF),
        vm((2, n, 2, half), BF), vm((2, n, 2, half), BF), vm((per, width), BF),
        vm((GROUPS, width), BF), vm((n, width), BF),
        dma((14,)),
        dma((sends,)), dma((n,)), dma((sends,)), dma((n,)), dma((sends,)), dma((n,)),
        dma((2,)), dma((2,)), dma, dma,
        dma((2, far, SUM_PIECES)), dma((2, far, SUM_PIECES)), dma, dma,
        dma((n - 1,)), dma((n,)),
        dma((2, far + 1, ROW_PIECES)), dma((2, far + 1, ROW_PIECES)),
        dma((2, far + 1, ROW_PIECES)), dma((2, far + 1, ROW_PIECES)),
        dma((2 * nz,)), dma((2 * nz,)),
        dma((2, far, BACK_PIECES)), dma((2, far, BACK_PIECES)),
        dma((2, n)), dma((2, n)),
    ]
    summed = pl.pallas_call(
        functools.partial(layer_kernel, (ny, nx, nz)),
        out_shape=jax.ShapeDtypeStruct(residual_in.shape, F32),
        in_specs=[ANY] * 14,
        out_specs=VM,
        scratch_shapes=scratch,
        compiler_params=pltpu.CompilerParams(
            collective_id=1, has_side_effects=True, vmem_limit_bytes=LIMIT
        ),
        name="layer",
    )(
        residual_in, queries, keys, values, break_offset.T, doc_ids[None, :], out_weight,
        norm_gain[None, :], group_router.T, expert_router.T, expert_ids.T, gate, up, down,
    )
    return summed.astype(BF)


def solution(mesh):
    n = mesh.shape["sp"]
    side = round(n**0.5)
    finer = Mesh(mesh.devices.reshape(side, n // side, mesh.shape["tp"] // 2, 2), AXES)
    in_specs = (
        P(SP + TP, None),
        P(SP, TP),
        P(SP, TP),
        P(SP, TP),
        P(SP, TP),
        P(SP),
        P(TP, None),
        P(),
        P(),
        P(),
        P(SP, None),
        P(SP, None, TP),
        P(SP, None, TP),
        P(SP, TP, None),
    )
    return jax.shard_map(
        per_device, mesh=finer, in_specs=in_specs, out_specs=P(SP + TP, None), check_vma=False
    )
```

```python
import functools

import jax
import jax.numpy as jnp
from jax import lax
from jax.experimental import pallas as pl
from jax.experimental.pallas import tpu as pltpu
from jax.sharding import Mesh
from jax.sharding import PartitionSpec as P

HEAD_DIM = 64
GROUPS = 2
DOC_MOST = 2560
KB = 256
BAND = DOC_MOST // KB
NEG = -1e30
SUM_PIECES = 4
ROW_PIECES = 4
BACK_PIECES = 4
NEAR = (0, 1, 3, 2)
MESH = pl.DeviceIdType.MESH
AXES = ("y", "x", "z", "c")
SP = ("y", "x")
TP = ("z", "c")
VM = pl.BlockSpec(memory_space=pltpu.VMEM)
ANY = pl.BlockSpec(memory_space=pl.ANY)
BF = jnp.bfloat16
F32 = jnp.float32
LIMIT = 60 * 1024 * 1024


def dot(a, b):
    return jnp.dot(a, b, preferred_element_type=F32)


def dot_t(a, b):
    return lax.dot_general(a, b, (((1,), (1,)), ((), ())), preferred_element_type=F32)


def iota(shape, axis):
    return lax.broadcasted_iota(jnp.int32, shape, axis)


def remote(src, dst, ss, rs, to):
    return pltpu.make_async_remote_copy(
        src_ref=src, dst_ref=dst, send_sem=ss, recv_sem=rs, device_id=to, device_id_type=MESH
    )


def attend_block(diag, q, kb, vb, ab, qd, part_out, part_go, later):
    heads = range(q.shape[1] // HEAD_DIM)
    rows = q.shape[0]
    cols = [slice(h * HEAD_DIM, (h + 1) * HEAD_DIM) for h in heads]
    scores = [dot_t(q[:, cols[h]], kb[:, cols[h]]) for h in heads]
    live = ab[len(heads) : len(heads) + 1, :].astype(F32) == qd[...]
    if diag:
        live = live & (iota((rows, KB), 1) < iota((rows, KB), 0))
    log_w, total = [], []
    for h in heads:
        s = jnp.where(live, scores[h] + ab[h : h + 1, :].astype(F32), NEG)
        go = jnp.maximum(s, 0.0) + jnp.log(1.0 + jnp.exp(-jnp.abs(s)))
        hi = go.astype(BF)
        lo = (go - hi.astype(F32)).astype(BF)
        total.append(jnp.sum(go, axis=1, keepdims=True))
        log_w.append((s - go, dot(hi, later[...]) + dot(lo, later[...])))
    for h in heads:
        o = dot(jnp.exp(log_w[h][0] - log_w[h][1]).astype(BF), vb[:, cols[h]])
        part_out[:, cols[h]] = o
        part_go[h] = total[h]


def layer_kernel(
    dims,
    res_, q_, k_, v_, off_, doc_, w, gain_, grp, exr, ids_, gate, up, down,
    out,
    res, q, k, v, off, doc, gain, ids,
    kall, vall, aall, auxo, later, qs, qd, acc, st, run, tot_out,
    wown, wsib, att, pair, part, sbb, rbb, xbuf, ybuf, mixed,
    sent, inb, rows, gw, uw, dw, dsib, hid, partc, sbc, rbc, fin, ret, back, grw, exw,
    lsem, ks, kr, vs, vr, as_, ar, ws, wr, ds, dr, bs, br, es, er,
    is_, ir, gs, gr, cs, cr, hs_, hr_, ss, rs, fs, fr,
):
    ny, nx, nz = dims
    y, x, z, c = (lax.axis_index(a) for a in AXES)
    me = y * nx + x
    n = ny * nx
    sib = (y, x, z, 1 - c)
    right = (y, x, lax.rem(z + 1, nz), c)
    left = (y, x, lax.rem(z + nz - 1, nz), c)
    half = wown.shape[1]
    heads = off.shape[0]
    own_half = pl.ds(pl.multiple_of(c * half, half), half)
    other_half = pl.ds(pl.multiple_of((1 - c) * half, half), half)
    far = nz // 2
    sends = []

    def start(q_):
        q_.start()
        sends.append(q_)

    others = []
    for dy in NEAR:
        for dx in range(nx):
            if dy or dx:
                ty, tx = lax.rem(y + dy, ny), lax.rem(x + dx, nx)
                others.append((ty, tx, ty * nx + tx))
    peers = [(ty, tx, z, c) for ty, tx, t in others]
    peers += [(ty, tx, z, 1 - c) for ty, tx, t in others]
    peers += [right, left, sib]
    bar = pltpu.get_barrier_semaphore()
    for p in peers:
        pl.semaphore_signal(bar, inc=1, device_id=p, device_id_type=MESH)
    small = [
        pltpu.make_async_copy(a, b, lsem.at[6 + i])
        for i, (a, b) in enumerate(
            [(off_, off), (doc_, doc), (k_, k), (v_, v), (q_, q), (ids_, ids), (gain_, gain), (res_, res)]
        )
    ]
    loads = [
        pltpu.make_async_copy(w.at[:, own_half], wown, lsem.at[0]),
        pltpu.make_async_copy(gate, gw, lsem.at[1]),
        pltpu.make_async_copy(up, uw, lsem.at[2]),
        pltpu.make_async_copy(down.at[:, own_half], dw, lsem.at[3]),
        pltpu.make_async_copy(grp, grw, lsem.at[4]),
        pltpu.make_async_copy(exr, exw, lsem.at[5]),
    ]
    for a in small + loads:
        a.start()

    later[...] = (iota((KB, KB), 0) > iota((KB, KB), 1)).astype(BF)
    for a in small:
        a.wait()
    docf = doc[...].astype(F32)
    eye = iota((KB, KB), 0) == iota((KB, KB), 1)
    qd[...] = jnp.sum(jnp.where(eye, docf, 0.0), axis=1, keepdims=True)
    pad = jnp.zeros((auxo.shape[0] - heads - 1, KB), F32)
    auxo[...] = jnp.concatenate([off[...].astype(F32), docf, pad], axis=0).astype(BF)
    qs[...] = q[...] * BF(HEAD_DIM**-0.5)
    pl.semaphore_wait(bar, len(peers))

    xs = [lax.rem(x + d, nx) for d in range(1, nx)]
    ys = [lax.rem(y + d, ny) for d in range(1, ny)]
    xb = [lax.rem(x + nx - d, nx) for d in range(1, nx)]
    yb = [lax.rem(y + ny - d, ny) for d in range(1, ny)]

    def used(b, j):
        return (j > b) & (j - b <= BAND)

    def k_first(src, dst):
        return (dst > src) | (y < ny - 1)

    def v_first(dst, src, col):
        return (dst > src) & (nx * (dst - src) - col <= BAND)

    def kcopy(b, src, asrc, i, to):
        return (
            remote(src, kall.at[b], ks.at[i], kr.at[b], to),
            remote(asrc, aall.at[b], as_.at[i], ar.at[b], to),
        )

    def vcopy(b, src, i, to):
        return (remote(src, vall.at[b], vs.at[i], vr.at[b], to),)

    plan = []

    def send(cond, copies):
        plan.append((cond, copies))

        @pl.when(cond)
        def _():
            for a in copies:
                a.start()

    def arrive(cond, copies):
        @pl.when(cond)
        def _():
            for a in copies:
                a.wait_recv()

    nk = nv = 0
    for a in xs:
        send(k_first(x, a), kcopy(me, k, auxo, nk, (y, a, z, c)))
        nk += 1
    for a in ys:
        send(v_first(a, y, x), vcopy(me, v, nv, (a, x, z, c)))
        nv += 1
    for a in ys:
        send(used(me, a * nx + x), kcopy(me, k, auxo, nk, (a, x, z, c)))
        nk += 1
    for a in xs:
        send(used(me, y * nx + a), vcopy(me, v, nv, (y, a, z, c)))
        nv += 1
    start(remote(w.at[:, other_half], wsib, ws.at[0], wr.at[0], sib))
    start(remote(down.at[:, other_half], dsib, ws.at[1], wr.at[1], sib))

    attend_block(True, qs, k, v, auxo, qd, acc.at[me], st.at[me], later)

    firsts = []
    for i in range(max(nx, ny) - 1):
        if i < nx - 1:
            b = y * nx + xb[i]
            got = k_first(xb[i], x)
            arrive(got, kcopy(b, k, auxo, 0, sib))
            for a in ys:
                send(got & used(b, a * nx + x), kcopy(b, kall.at[b], aall.at[b], nk, (a, x, z, c)))
                nk += 1
        if i < ny - 1:
            b = yb[i] * nx + x
            got = v_first(y, yb[i], x)
            arrive(got, vcopy(b, v, 0, sib))
            for a in xs:
                send(got & used(b, y * nx + a), vcopy(b, vall.at[b], nv, (y, a, z, c)))
                nv += 1
    del firsts

    def step(b):
        by = lax.div(b, nx)
        bx = lax.rem(b, nx)

        @pl.when(by != y)
        def _():
            for a in kcopy(b, k, auxo, 0, sib):
                a.wait_recv()

        @pl.when(bx != x)
        def _():
            for a in vcopy(b, v, 0, sib):
                a.wait_recv()

        attend_block(
            False, qs, kall.at[b], vall.at[b], aall.at[b], qd, acc.at[b], st.at[b], later
        )

    def walk(i, carry):
        b = (y - lax.rem(i, ny)) * nx + lax.rem(x + nx - lax.div(i, ny), nx)

        @pl.when((b >= 0) & used(b, me))
        def _():
            step(b)

        return carry

    lax.fori_loop(1, n, walk, 0)
    run[...] = st[me]
    tot_out[...] = acc[me]

    def gather(t, carry):
        b = me - t
        for h in range(heads):
            hs = slice(h * HEAD_DIM, (h + 1) * HEAD_DIM)
            before = run[h]
            tot_out[:, hs] = tot_out[:, hs] + jnp.exp(-before) * acc[b, :, hs]
            run[h] = before + st[b, h]
        return carry

    lax.fori_loop(1, jnp.minimum(me, BAND) + 1, gather, 0)
    att[...] = tot_out[...].astype(BF)
    swap = remote(att, pair, ds, dr, sib)
    start(swap)

    def ring_sum(own, sbuf, rbuf, s_sem, r_sem, np_, hr, last, begun=None):
        def move(d, s, p):
            ref = (d, s, pl.ds(p * hr, hr))
            return remote(
                sbuf.at[ref], rbuf.at[ref], s_sem.at[d, s, p], r_sem.at[d, s, p],
                right if d == 0 else left,
            )

        def half_of(d):
            return range(np_ // 2) if d == 0 else range(np_ // 2, np_)

        for s in range(far) if begun is not False else (1,):
            for i in range(np_ // 2 if s == 0 or (s == 1 and begun is not None) else np_):
                for d in range(2):
                    order = list(half_of(d)) + ([] if s == 0 else list(half_of(1 - d)))
                    p = order[i] if begun is not False else half_of(1 - d)[i]
                    dist = far - s
                    zz = lax.rem(z + dist, nz) if d == 0 else lax.rem(z + nz - dist, nz)
                    val = own(zz, p)
                    if s > 1 or (s == 1 and p in half_of(d)):
                        move(d, s - 1, p).wait_recv()
                        val = val + rbuf[d, s - 1, p * hr : (p + 1) * hr, :].astype(F32)
                    sbuf[d, s, p * hr : (p + 1) * hr, :] = val.astype(BF)
                    start(move(d, s, p))
        if begun is False:
            return
        for i in range(np_):
            p = i
            for d in range(2):
                move(d, far - 1, p).wait_recv()
            tot = own(z, p)
            for d in range(2):
                tot = tot + rbuf[d, far - 1, p * hr : (p + 1) * hr, :].astype(F32)
            last(p, tot)

    chunk = part.shape[0] // nz
    hr = chunk // SUM_PIECES
    loads[0].wait()
    part[...] = dot(att[...], wown[...])
    remote(w.at[:, other_half], wsib, ws.at[0], wr.at[0], sib).wait_recv()
    swap.wait_recv()
    part[...] += dot(pair[...], wsib[...])

    def own_b(zz, p):
        return part[pl.ds(pl.multiple_of(zz * chunk + p * hr, hr), hr), :]

    crow = chunk // 2

    def last_b(p, tot):
        for i in range(max(1, hr // crow)):
            r = p * hr + i * crow if hr >= crow else p * hr
            cnt = min(hr, crow)
            core = r // crow
            at = r % crow
            piece = tot[i * crow : i * crow + cnt] if hr >= crow else tot

            @pl.when(c == core)
            def _():
                ybuf[c, at : at + cnt, :] = piece

            @pl.when(c != core)
            def _():
                xbuf[at : at + cnt, :] = piece

    ring_sum(own_b, sbb, rbb, bs, br, SUM_PIECES, hr, last_b)
    trade = remote(xbuf, ybuf.at[c], es, er, sib)
    start(trade)
    remote(xbuf, ybuf.at[1 - c], es, er, sib).wait_recv()
    lo = res[:, :half].astype(F32) + ybuf[0]
    hi = res[:, half:].astype(F32) + ybuf[1]
    mlo, mhi = lo.astype(BF), hi.astype(BF)
    mixed[:, :half] = mlo
    mixed[:, half:] = mhi
    lo, hi = mlo.astype(F32), mhi.astype(F32)
    mean = (
        jnp.sum(lo * lo, axis=1, keepdims=True) + jnp.sum(hi * hi, axis=1, keepdims=True)
    ) / (2 * half)
    scale = lax.rsqrt(mean + 1e-06)
    nlo = (lo * scale * gain[:, :half]).astype(BF)
    nhi = (hi * scale * gain[:, half:]).astype(BF)

    tok = res.shape[0]
    here = iota((tok, KB), 1) == (z * 2 + c) * tok + iota((tok, KB), 0)
    chosen = [
        jnp.sum(jnp.where(here, ids[i : i + 1, :], 0), axis=1, keepdims=True) for i in range(2)
    ]
    eye16 = iota((tok, tok), 0) == iota((tok, tok), 1)
    trow = [
        jnp.sum(jnp.where(eye16, chosen[i], 0), axis=0, keepdims=True)
        for i in range(2)
    ]
    slot = iota((2 * n, tok), 0)
    expert_of = lax.div(slot, 2)
    named = ((trow[0] == expert_of) | (trow[1] == expert_of)).astype(F32)
    earlier = (iota((tok, tok), 0) < iota((tok, tok), 1)).astype(BF)
    rank = dot(named.astype(BF), earlier)
    odd = lax.rem(slot, 2).astype(F32)
    pick = jnp.where(rank == odd, named, 0.0).astype(BF)
    slo = dot(pick, nlo).astype(BF)
    shi = dot(pick, nhi).astype(BF)
    for e in range(n):
        sent[e, :, :half] = slo[2 * e : 2 * e + 2, :]
        sent[e, :, half:] = shi[2 * e : 2 * e + 2, :]

    for d, (ty, tx, t) in enumerate(others):
        start(remote(sent.at[t], inb.at[me], is_.at[d], ir.at[me], (ty, tx, z, c)))
    inb[me] = sent[me]

    normed = jnp.concatenate([nlo, nhi], axis=1)
    loads[4].wait()
    loads[5].wait()
    glog = dot_t(normed, grw[...])
    elog = dot_t(normed, exw[...])
    margin = glog[:, 0:1] - glog[:, 1:2]
    own_margin = jnp.where(chosen[0] < n // GROUPS, margin, -margin)
    share = jax.nn.sigmoid(own_margin)
    eid = iota((tok, n), 1)
    picked = [
        jnp.sum(jnp.where(chosen[i] == eid, elog, 0.0), axis=1, keepdims=True)
        for i in range(2)
    ]
    route = [share * jax.nn.sigmoid(picked[i] - picked[1 - i]) for i in range(2)]
    slot_c = iota((tok, 2 * n), 1)
    exp_c = lax.div(slot_c, 2)
    is_k = [chosen[i] == exp_c for i in range(2)]
    named_c = (is_k[0] | is_k[1]).astype(BF)
    before = (iota((tok, tok), 1) < iota((tok, tok), 0)).astype(BF)
    rank_c = dot(before, named_c)
    odd_c = lax.rem(slot_c, 2).astype(F32)
    take = [
        jnp.where(is_k[i] & (rank_c == odd_c), 1.0, 0.0).astype(BF) for i in range(2)
    ]

    mine = z * 2 + c

    per = rows.shape[1]
    hb = per // ROW_PIECES

    def spot(p):
        return pl.multiple_of(lax.rem(y + NEAR[p], ny) * hb, hb)

    def piece(b, p):
        return rows.at[b, pl.ds(spot(p), hb), :]

    def from_chip(d, h):
        return lax.rem(z + nz - h, nz) if d == 0 else lax.rem(z + h, nz)

    def hop(d, h, p):
        b = from_chip(d, h - 1) * 2 + c
        return remote(
            piece(b, p), piece(b, p), gs.at[d, h, p], gr.at[d, h, p], right if d == 0 else left
        )

    def got_hop(d, h, p):
        b = from_chip(d, h) * 2 + c
        return remote(piece(b, p), piece(b, p), gs.at[d, h, p], gr.at[d, h, p], sib)

    def cross(d, h, p, core):
        b = from_chip(d, h) * 2 + core
        return remote(piece(b, p), piece(b, p), cs.at[d, h, p], cr.at[d, h, p], sib)

    def pieces(d, h):
        if h < far:
            return list(range(ROW_PIECES))
        hp = ROW_PIECES // 2
        return list(range(hp)) if d == 0 else list(range(hp, ROW_PIECES))

    def order(d):
        return (0, 1, 2, 3) if d == 0 else (0, 2, 3, 1)

    def out_pieces(k):
        return [(0, k)] + {0: [(1, 0)], 1: [], 2: [(1, 2)], 3: [(1, 3), (1, 1)]}[k]

    for p in range(ROW_PIECES):
        ty = lax.rem(y + NEAR[p], ny)
        for dx in range(nx):
            if NEAR[p] or dx:
                t = ty * nx + lax.rem(x + dx, nx)
                remote(sent.at[t], inb.at[t], is_.at[0], ir.at[t], sib).wait_recv()
        rows[mine, pl.ds(spot(p), hb), :] = jnp.concatenate(
            [inb[ty * nx + q_] for q_ in range(nx)], axis=0
        )
        for d, k_ in out_pieces(p):
            start(hop(d, 1, k_))
        start(cross(0, 0, p, c))

    def blocks_of(h):
        if h == 0:
            return [(z * 2 + i, i) for i in (0, 1)]
        lo_ = from_chip(0, h)
        hi_ = from_chip(1, h)
        if h == far:
            return [(lo_ * 2 + i, 4 * h - 2 + i) for i in (0, 1)]
        return [(lo_ * 2 + i, 4 * h - 2 + i) for i in (0, 1)] + [
            (hi_ * 2 + i, 4 * h + i) for i in (0, 1)
        ]

    def hswap(b, i):
        return remote(hid.at[0, b], hid.at[1, b], hs_.at[i], hr_.at[i], sib)

    def run(h):
        for d in (0, 1):
            if h == 0 and d == 1:
                continue
            for p in pieces(d, h):
                cross(d, h, p, 1 - c).wait_recv()
        bl = blocks_of(h)
        xin = jnp.concatenate([rows[b] for b, i in bl], axis=0)
        g = dot(xin, gw[...])
        u = dot(xin, uw[...])
        hv = (g * jax.nn.sigmoid(g) * u).astype(BF)
        for j, (b, i) in enumerate(bl):
            hid[0, b] = hv[j * per : (j + 1) * per]
            start(hswap(b, i))

    def finish(h):
        bl = blocks_of(h)
        for b, i in bl:
            hswap(b, i).wait_recv()
        h0 = jnp.concatenate([hid[0, b] for b, i in bl], axis=0)
        h1 = jnp.concatenate([hid[1, b] for b, i in bl], axis=0)
        val = dot(h0, dw[...]) + dot(h1, dsib[...])
        for j, (b, i) in enumerate(bl):
            partc[b] = val[j * per : (j + 1) * per]

    loads[1].wait()
    loads[2].wait()
    for h in range(1, far + 1):
        for i in range(ROW_PIECES):
            for d in (0, 1):
                p = order(d)[i]
                if p not in pieces(d, h):
                    continue
                got_hop(d, h, p).wait_recv()
                if h + 1 <= far and p in pieces(d, h + 1):
                    start(hop(d, h + 1, p))
                start(cross(d, h, p, c))
            if i == 0:
                run(h - 1)
                if h == 1:
                    loads[3].wait()
                    remote(down.at[:, other_half], dsib, ws.at[1], wr.at[1], sib).wait_recv()
            if i == 1:
                finish(h - 1)
    chunk_c = 2 * per
    hc = chunk_c // BACK_PIECES

    def own_c(zz, p):
        b = zz * 2 + (p * hc) // per
        return partc[b, (p * hc) % per : (p * hc) % per + hc, :]

    def last_c(p, tot):
        core = (p * hc) // per
        e0 = ((p * hc) % per) // 2
        tb = tot.astype(BF)
        for e in range(hc // 2):
            t = e0 + e
            fin[core, t] = tb[2 * e : 2 * e + 2, :]
            ty, tx = t // nx, t % nx

            @pl.when(me != t)
            def _(t=t, ty=ty, tx=tx):
                remote(
                    fin.at[core, t], ret.at[c, me], fs.at[core, t], fr.at[c, me], (ty, tx, z, core)
                ).start()

            @pl.when((me == t) & (c != core))
            def _(t=t):
                remote(
                    fin.at[core, t], ret.at[c, me], fs.at[core, t], fr.at[c, me], sib
                ).start()

    back_ring = (own_c, sbc, rbc, ss, rs, BACK_PIECES, hc, last_c)
    ring_sum(*back_ring, begun=False)
    run(far)
    finish(far)
    ring_sum(*back_ring, begun=True)
    ret[c, me] = fin[c, me]
    for i in (0, 1):
        for t in range(n):

            @pl.when((me != t) | (c != i))
            def _(t=t, i=i):
                remote(fin.at[0, t], ret.at[i, t], fs.at[0, t], fr.at[i, t], sib).wait_recv()

            back[2 * t : 2 * t + 2, i * half : (i + 1) * half] = ret[i, t]
    for i in range(2):
        cols = slice(i * half, (i + 1) * half)
        bk = back[:, cols]
        mix = route[0] * dot(take[0], bk) + route[1] * dot(take[1], bk)
        out[:, cols] = mixed[:, cols].astype(F32) + mix

    for cond, copies in plan:

        @pl.when(cond)
        def _(copies=copies):
            for a in copies:
                a.wait_send()

    for core in (0, 1):
        for t in range(n):

            @pl.when((me != t) | (c != core))
            def _(t=t, core=core):
                remote(
                    fin.at[core, t], ret.at[c, me], fs.at[core, t], fr.at[c, me], sib
                ).wait_send()

    for a in sends:
        a.wait_send()


def per_device(
    residual_in, queries, keys, values, break_offset, doc_ids, out_weight, norm_gain,
    group_router, expert_router, expert_ids, gate_weight, up_weight, down_weight,
):
    ny, nx, nz = lax.axis_size("y"), lax.axis_size("x"), lax.axis_size("z")
    n = ny * nx
    rows, att = queries.shape
    tok, width = residual_in.shape
    half = width // 2
    heads = break_offset.shape[1]
    gate, up, down = gate_weight[0], up_weight[0], down_weight[0]
    units = gate.shape[1]
    per = 2 * n
    far = nz // 2
    sends = (nx - 1) + (ny - 1) + (nx - 1) * (ny - 1)
    dma = pltpu.SemaphoreType.DMA
    vm = pltpu.VMEM
    scratch = [
        vm((tok, width), BF), vm((rows, att), BF), vm((rows, att), BF), vm((rows, att), BF),
        vm((heads, rows), BF), vm((1, rows), jnp.int32), vm((1, width), F32),
        vm((2, rows), jnp.int32),
        vm((n, rows, att), BF), vm((n, rows, att), BF), vm((n, 16, rows), BF), vm((16, rows), BF),
        vm((KB, KB), BF), vm((rows, att), BF), vm((rows, 1), F32), vm((n, rows, att), F32),
        vm((n, heads, rows, 1), F32), vm((heads, rows, 1), F32), vm((rows, att), F32),
        vm((att, half), BF), vm((att, half), BF), vm((rows, att), BF), vm((rows, att), BF),
        vm((rows, half), F32),
        vm((2, far, rows // nz, half), BF), vm((2, far, rows // nz, half), BF),
        vm((tok, half), F32), vm((2, tok, half), F32), vm((tok, width), BF),
        vm((n, 2, width), BF), vm((n, 2, width), BF), vm((2 * nz, per, width), BF),
        vm((width, units), BF), vm((width, units), BF), vm((units, half), BF),
        vm((units, half), BF),
        vm((2, 2 * nz, per, units), BF), vm((2 * nz, per, half), F32),
        vm((2, far, 2 * per, half), BF), vm((2, far, 2 * per, half), BF),
        vm((2, n, 2, half), BF), vm((2, n, 2, half), BF), vm((per, width), BF),
        vm((GROUPS, width), BF), vm((n, width), BF),
        dma((14,)),
        dma((sends,)), dma((n,)), dma((sends,)), dma((n,)), dma((sends,)), dma((n,)),
        dma((2,)), dma((2,)), dma, dma,
        dma((2, far, SUM_PIECES)), dma((2, far, SUM_PIECES)), dma, dma,
        dma((n - 1,)), dma((n,)),
        dma((2, far + 1, ROW_PIECES)), dma((2, far + 1, ROW_PIECES)),
        dma((2, far + 1, ROW_PIECES)), dma((2, far + 1, ROW_PIECES)),
        dma((2 * nz,)), dma((2 * nz,)),
        dma((2, far, BACK_PIECES)), dma((2, far, BACK_PIECES)),
        dma((2, n)), dma((2, n)),
    ]
    summed = pl.pallas_call(
        functools.partial(layer_kernel, (ny, nx, nz)),
        out_shape=jax.ShapeDtypeStruct(residual_in.shape, F32),
        in_specs=[ANY] * 14,
        out_specs=VM,
        scratch_shapes=scratch,
        compiler_params=pltpu.CompilerParams(
            collective_id=1, has_side_effects=True, vmem_limit_bytes=LIMIT
        ),
        name="layer",
    )(
        residual_in, queries, keys, values, break_offset.T, doc_ids[None, :], out_weight,
        norm_gain[None, :], group_router.T, expert_router.T, expert_ids.T, gate, up, down,
    )
    return summed.astype(BF)


def solution(mesh):
    n = mesh.shape["sp"]
    side = round(n**0.5)
    finer = Mesh(mesh.devices.reshape(side, n // side, mesh.shape["tp"] // 2, 2), AXES)
    in_specs = (
        P(SP + TP, None),
        P(SP, TP),
        P(SP, TP),
        P(SP, TP),
        P(SP, TP),
        P(SP),
        P(TP, None),
        P(),
        P(),
        P(),
        P(SP, None),
        P(SP, None, TP),
        P(SP, None, TP),
        P(SP, TP, None),
    )
    return jax.shard_map(
        per_device, mesh=finer, in_specs=in_specs, out_specs=P(SP + TP, None), check_vma=False
    )
```

```python
import functools

import jax
import jax.numpy as jnp
from jax import lax
from jax.experimental import pallas as pl
from jax.experimental.pallas import tpu as pltpu
from jax.sharding import Mesh
from jax.sharding import PartitionSpec as P

HEAD_DIM = 64
GROUPS = 2
DOC_MOST = 2560
KB = 256
BAND = DOC_MOST // KB
NEG = -1e30
SUM_PIECES = 4
ROW_PIECES = 4
BACK_PIECES = 4
NEAR = (0, 1, 3, 2)
MESH = pl.DeviceIdType.MESH
AXES = ("y", "x", "z", "c")
SP = ("y", "x")
TP = ("z", "c")
VM = pl.BlockSpec(memory_space=pltpu.VMEM)
ANY = pl.BlockSpec(memory_space=pl.ANY)
BF = jnp.bfloat16
F32 = jnp.float32
LIMIT = 60 * 1024 * 1024


def dot(a, b):
    return jnp.dot(a, b, preferred_element_type=F32)


def dot_t(a, b):
    return lax.dot_general(a, b, (((1,), (1,)), ((), ())), preferred_element_type=F32)


def iota(shape, axis):
    return lax.broadcasted_iota(jnp.int32, shape, axis)


def remote(src, dst, ss, rs, to):
    return pltpu.make_async_remote_copy(
        src_ref=src, dst_ref=dst, send_sem=ss, recv_sem=rs, device_id=to, device_id_type=MESH
    )


def attend_block(diag, q, kb, vb, ab, qd, part_out, part_go, later):
    heads = range(q.shape[1] // HEAD_DIM)
    rows = q.shape[0]
    cols = [slice(h * HEAD_DIM, (h + 1) * HEAD_DIM) for h in heads]
    scores = [dot_t(q[:, cols[h]], kb[:, cols[h]]) for h in heads]
    live = ab[len(heads) : len(heads) + 1, :].astype(F32) == qd[...]
    if diag:
        live = live & (iota((rows, KB), 1) < iota((rows, KB), 0))
    log_w, total = [], []
    for h in heads:
        s = jnp.where(live, scores[h] + ab[h : h + 1, :].astype(F32), NEG)
        go = jnp.maximum(s, 0.0) + jnp.log(1.0 + jnp.exp(-jnp.abs(s)))
        hi = go.astype(BF)
        lo = (go - hi.astype(F32)).astype(BF)
        total.append(jnp.sum(go, axis=1, keepdims=True))
        log_w.append((s - go, dot(hi, later[...]) + dot(lo, later[...])))
    for h in heads:
        o = dot(jnp.exp(log_w[h][0] - log_w[h][1]).astype(BF), vb[:, cols[h]])
        part_out[:, cols[h]] = o
        part_go[h] = total[h]


def layer_kernel(
    dims,
    res_, q_, k_, v_, off_, doc_, w, gain_, grp, exr, ids_, gate, up, down,
    out,
    res, q, k, v, off, doc, gain, ids,
    kall, vall, aall, auxo, later, qs, qd, acc, st, run, tot_out,
    wown, wsib, att, pair, part, sbb, rbb, xbuf, ybuf, mixed,
    sent, inb, rows, gw, uw, dw, dsib, hid, partc, sbc, rbc, fin, ret, back, grw, exw,
    lsem, ks, kr, vs, vr, as_, ar, ws, wr, ds, dr, bs, br, es, er,
    is_, ir, gs, gr, cs, cr, hs_, hr_, ss, rs, fs, fr,
):
    ny, nx, nz = dims
    y, x, z, c = (lax.axis_index(a) for a in AXES)
    me = y * nx + x
    n = ny * nx
    sib = (y, x, z, 1 - c)
    right = (y, x, lax.rem(z + 1, nz), c)
    left = (y, x, lax.rem(z + nz - 1, nz), c)
    half = wown.shape[1]
    heads = off.shape[0]
    own_half = pl.ds(pl.multiple_of(c * half, half), half)
    other_half = pl.ds(pl.multiple_of((1 - c) * half, half), half)
    far = nz // 2
    sends = []

    def start(q_):
        q_.start()
        sends.append(q_)

    others = []
    for dy in NEAR:
        for dx in range(nx):
            if dy or dx:
                ty, tx = lax.rem(y + dy, ny), lax.rem(x + dx, nx)
                others.append((ty, tx, ty * nx + tx))
    peers = [(ty, tx, z, c) for ty, tx, t in others]
    peers += [(ty, tx, z, 1 - c) for ty, tx, t in others]
    peers += [right, left, sib]
    bar = pltpu.get_barrier_semaphore()
    for p in peers:
        pl.semaphore_signal(bar, inc=1, device_id=p, device_id_type=MESH)
    small = [
        pltpu.make_async_copy(a, b, lsem.at[6 + i])
        for i, (a, b) in enumerate(
            [(off_, off), (doc_, doc), (k_, k), (v_, v), (q_, q), (ids_, ids), (gain_, gain), (res_, res)]
        )
    ]
    loads = [
        pltpu.make_async_copy(w.at[:, own_half], wown, lsem.at[0]),
        pltpu.make_async_copy(gate, gw, lsem.at[1]),
        pltpu.make_async_copy(up, uw, lsem.at[2]),
        pltpu.make_async_copy(down.at[:, own_half], dw, lsem.at[3]),
        pltpu.make_async_copy(grp, grw, lsem.at[4]),
        pltpu.make_async_copy(exr, exw, lsem.at[5]),
    ]
    for a in small + loads:
        a.start()

    later[...] = (iota((KB, KB), 0) > iota((KB, KB), 1)).astype(BF)
    for a in small:
        a.wait()
    docf = doc[...].astype(F32)
    eye = iota((KB, KB), 0) == iota((KB, KB), 1)
    qd[...] = jnp.sum(jnp.where(eye, docf, 0.0), axis=1, keepdims=True)
    pad = jnp.zeros((auxo.shape[0] - heads - 1, KB), F32)
    auxo[...] = jnp.concatenate([off[...].astype(F32), docf, pad], axis=0).astype(BF)
    qs[...] = q[...] * BF(HEAD_DIM**-0.5)
    pl.semaphore_wait(bar, len(peers))

    xs = [lax.rem(x + d, nx) for d in range(1, nx)]
    ys = [lax.rem(y + d, ny) for d in range(1, ny)]
    xb = [lax.rem(x + nx - d, nx) for d in range(1, nx)]
    yb = [lax.rem(y + ny - d, ny) for d in range(1, ny)]

    def used(b, j):
        return (j > b) & (j - b <= BAND)

    def k_first(src, dst):
        return (dst > src) | (y < ny - 1)

    def v_first(dst, src, col):
        return (dst > src) & (nx * (dst - src) - col <= BAND)

    def kcopy(b, src, asrc, i, to):
        return (
            remote(src, kall.at[b], ks.at[i], kr.at[b], to),
            remote(asrc, aall.at[b], as_.at[i], ar.at[b], to),
        )

    def vcopy(b, src, i, to):
        return (remote(src, vall.at[b], vs.at[i], vr.at[b], to),)

    plan = []

    def send(cond, copies):
        plan.append((cond, copies))

        @pl.when(cond)
        def _():
            for a in copies:
                a.start()

    def arrive(cond, copies):
        @pl.when(cond)
        def _():
            for a in copies:
                a.wait_recv()

    nk = nv = 0
    for a in xs:
        send(k_first(x, a), kcopy(me, k, auxo, nk, (y, a, z, c)))
        nk += 1
    for a in ys:
        send(v_first(a, y, x), vcopy(me, v, nv, (a, x, z, c)))
        nv += 1
    for a in ys:
        send(used(me, a * nx + x), kcopy(me, k, auxo, nk, (a, x, z, c)))
        nk += 1
    for a in xs:
        send(used(me, y * nx + a), vcopy(me, v, nv, (y, a, z, c)))
        nv += 1
    start(remote(w.at[:, other_half], wsib, ws.at[0], wr.at[0], sib))
    start(remote(down.at[:, other_half], dsib, ws.at[1], wr.at[1], sib))

    attend_block(True, qs, k, v, auxo, qd, acc.at[me], st.at[me], later)

    firsts = []
    for i in range(max(nx, ny) - 1):
        if i < nx - 1:
            b = y * nx + xb[i]
            got = k_first(xb[i], x)
            arrive(got, kcopy(b, k, auxo, 0, sib))
            for a in ys:
                send(got & used(b, a * nx + x), kcopy(b, kall.at[b], aall.at[b], nk, (a, x, z, c)))
                nk += 1
        if i < ny - 1:
            b = yb[i] * nx + x
            got = v_first(y, yb[i], x)
            arrive(got, vcopy(b, v, 0, sib))
            for a in xs:
                send(got & used(b, y * nx + a), vcopy(b, vall.at[b], nv, (y, a, z, c)))
                nv += 1
    del firsts

    def step(b):
        by = lax.div(b, nx)
        bx = lax.rem(b, nx)

        @pl.when(by != y)
        def _():
            for a in kcopy(b, k, auxo, 0, sib):
                a.wait_recv()

        @pl.when(bx != x)
        def _():
            for a in vcopy(b, v, 0, sib):
                a.wait_recv()

        attend_block(
            False, qs, kall.at[b], vall.at[b], aall.at[b], qd, acc.at[b], st.at[b], later
        )

    def walk(i, carry):
        b = (y - lax.rem(i, ny)) * nx + lax.rem(x + nx - lax.div(i, ny), nx)

        @pl.when((b >= 0) & used(b, me))
        def _():
            step(b)

        return carry

    lax.fori_loop(1, n, walk, 0)
    run[...] = st[me]
    tot_out[...] = acc[me]

    def gather(t, carry):
        b = me - t
        for h in range(heads):
            hs = slice(h * HEAD_DIM, (h + 1) * HEAD_DIM)
            before = run[h]
            tot_out[:, hs] = tot_out[:, hs] + jnp.exp(-before) * acc[b, :, hs]
            run[h] = before + st[b, h]
        return carry

    lax.fori_loop(1, jnp.minimum(me, BAND) + 1, gather, 0)
    att[...] = tot_out[...].astype(BF)
    swap = remote(att, pair, ds, dr, sib)
    start(swap)

    def ring_sum(own, sbuf, rbuf, s_sem, r_sem, np_, hr, last, begun=None):
        def move(d, s, p):
            ref = (d, s, pl.ds(p * hr, hr))
            return remote(
                sbuf.at[ref], rbuf.at[ref], s_sem.at[d, s, p], r_sem.at[d, s, p],
                right if d == 0 else left,
            )

        def half_of(d):
            return range(np_ // 2) if d == 0 else range(np_ // 2, np_)

        for s in range(far) if begun is not False else (1,):
            for i in range(np_ // 2 if s == 0 or (s == 1 and begun is not None) else np_):
                for d in range(2):
                    chained, fresh = list(half_of(d)), list(half_of(1 - d))
                    if s == 0 or (s == 1 and begun):
                        p = chained[i]
                    else:
                        p = (fresh + chained)[i]
                    dist = far - s
                    zz = lax.rem(z + dist, nz) if d == 0 else lax.rem(z + nz - dist, nz)
                    val = own(zz, p)
                    if s > 1 or (s == 1 and p in half_of(d)):
                        move(d, s - 1, p).wait_recv()
                        val = val + rbuf[d, s - 1, p * hr : (p + 1) * hr, :].astype(F32)
                    sbuf[d, s, p * hr : (p + 1) * hr, :] = val.astype(BF)
                    start(move(d, s, p))
        if begun is False:
            return
        for i in range(np_):
            p = i
            for d in range(2):
                move(d, far - 1, p).wait_recv()
            tot = own(z, p)
            for d in range(2):
                tot = tot + rbuf[d, far - 1, p * hr : (p + 1) * hr, :].astype(F32)
            last(p, tot)

    chunk = part.shape[0] // nz
    hr = chunk // SUM_PIECES
    loads[0].wait()
    part[...] = dot(att[...], wown[...])
    remote(w.at[:, other_half], wsib, ws.at[0], wr.at[0], sib).wait_recv()
    swap.wait_recv()
    part[...] += dot(pair[...], wsib[...])

    def own_b(zz, p):
        return part[pl.ds(pl.multiple_of(zz * chunk + p * hr, hr), hr), :]

    crow = chunk // 2

    def last_b(p, tot):
        for i in range(max(1, hr // crow)):
            r = p * hr + i * crow if hr >= crow else p * hr
            cnt = min(hr, crow)
            core = r // crow
            at = r % crow
            piece = tot[i * crow : i * crow + cnt] if hr >= crow else tot

            @pl.when(c == core)
            def _():
                ybuf[c, at : at + cnt, :] = piece

            @pl.when(c != core)
            def _():
                xbuf[at : at + cnt, :] = piece

    ring_sum(own_b, sbb, rbb, bs, br, SUM_PIECES, hr, last_b)
    trade = remote(xbuf, ybuf.at[c], es, er, sib)
    start(trade)
    remote(xbuf, ybuf.at[1 - c], es, er, sib).wait_recv()
    lo = res[:, :half].astype(F32) + ybuf[0]
    hi = res[:, half:].astype(F32) + ybuf[1]
    mlo, mhi = lo.astype(BF), hi.astype(BF)
    mixed[:, :half] = mlo
    mixed[:, half:] = mhi
    lo, hi = mlo.astype(F32), mhi.astype(F32)
    mean = (
        jnp.sum(lo * lo, axis=1, keepdims=True) + jnp.sum(hi * hi, axis=1, keepdims=True)
    ) / (2 * half)
    scale = lax.rsqrt(mean + 1e-06)
    nlo = (lo * scale * gain[:, :half]).astype(BF)
    nhi = (hi * scale * gain[:, half:]).astype(BF)

    tok = res.shape[0]
    here = iota((tok, KB), 1) == (z * 2 + c) * tok + iota((tok, KB), 0)
    chosen = [
        jnp.sum(jnp.where(here, ids[i : i + 1, :], 0), axis=1, keepdims=True) for i in range(2)
    ]
    eye16 = iota((tok, tok), 0) == iota((tok, tok), 1)
    trow = [
        jnp.sum(jnp.where(eye16, chosen[i], 0), axis=0, keepdims=True)
        for i in range(2)
    ]
    slot = iota((2 * n, tok), 0)
    expert_of = lax.div(slot, 2)
    named = ((trow[0] == expert_of) | (trow[1] == expert_of)).astype(F32)
    earlier = (iota((tok, tok), 0) < iota((tok, tok), 1)).astype(BF)
    rank = dot(named.astype(BF), earlier)
    odd = lax.rem(slot, 2).astype(F32)
    pick = jnp.where(rank == odd, named, 0.0).astype(BF)
    slo = dot(pick, nlo).astype(BF)
    shi = dot(pick, nhi).astype(BF)
    for e in range(n):
        sent[e, :, :half] = slo[2 * e : 2 * e + 2, :]
        sent[e, :, half:] = shi[2 * e : 2 * e + 2, :]

    for d, (ty, tx, t) in enumerate(others):
        start(remote(sent.at[t], inb.at[me], is_.at[d], ir.at[me], (ty, tx, z, c)))
    inb[me] = sent[me]

    normed = jnp.concatenate([nlo, nhi], axis=1)
    loads[4].wait()
    loads[5].wait()
    glog = dot_t(normed, grw[...])
    elog = dot_t(normed, exw[...])
    margin = glog[:, 0:1] - glog[:, 1:2]
    own_margin = jnp.where(chosen[0] < n // GROUPS, margin, -margin)
    share = jax.nn.sigmoid(own_margin)
    eid = iota((tok, n), 1)
    picked = [
        jnp.sum(jnp.where(chosen[i] == eid, elog, 0.0), axis=1, keepdims=True)
        for i in range(2)
    ]
    route = [share * jax.nn.sigmoid(picked[i] - picked[1 - i]) for i in range(2)]
    slot_c = iota((tok, 2 * n), 1)
    exp_c = lax.div(slot_c, 2)
    is_k = [chosen[i] == exp_c for i in range(2)]
    named_c = (is_k[0] | is_k[1]).astype(BF)
    before = (iota((tok, tok), 1) < iota((tok, tok), 0)).astype(BF)
    rank_c = dot(before, named_c)
    odd_c = lax.rem(slot_c, 2).astype(F32)
    take = [
        jnp.where(is_k[i] & (rank_c == odd_c), 1.0, 0.0).astype(BF) for i in range(2)
    ]

    mine = z * 2 + c

    per = rows.shape[1]
    hb = per // ROW_PIECES

    def spot(p):
        return pl.multiple_of(lax.rem(y + NEAR[p], ny) * hb, hb)

    def piece(b, p):
        return rows.at[b, pl.ds(spot(p), hb), :]

    def from_chip(d, h):
        return lax.rem(z + nz - h, nz) if d == 0 else lax.rem(z + h, nz)

    def hop(d, h, p):
        b = from_chip(d, h - 1) * 2 + c
        return remote(
            piece(b, p), piece(b, p), gs.at[d, h, p], gr.at[d, h, p], right if d == 0 else left
        )

    def got_hop(d, h, p):
        b = from_chip(d, h) * 2 + c
        return remote(piece(b, p), piece(b, p), gs.at[d, h, p], gr.at[d, h, p], sib)

    def cross(d, h, p, core):
        b = from_chip(d, h) * 2 + core
        return remote(piece(b, p), piece(b, p), cs.at[d, h, p], cr.at[d, h, p], sib)

    def pieces(d, h):
        if h < far:
            return list(range(ROW_PIECES))
        hp = ROW_PIECES // 2
        return list(range(hp)) if d == 0 else list(range(hp, ROW_PIECES))

    def order(d):
        return (0, 1, 2, 3) if d == 0 else (0, 2, 3, 1)

    def out_pieces(k):
        return [(0, k)] + {0: [(1, 0)], 1: [], 2: [(1, 2)], 3: [(1, 3), (1, 1)]}[k]

    for p in range(ROW_PIECES):
        ty = lax.rem(y + NEAR[p], ny)
        for dx in range(nx):
            if NEAR[p] or dx:
                t = ty * nx + lax.rem(x + dx, nx)
                remote(sent.at[t], inb.at[t], is_.at[0], ir.at[t], sib).wait_recv()
        rows[mine, pl.ds(spot(p), hb), :] = jnp.concatenate(
            [inb[ty * nx + q_] for q_ in range(nx)], axis=0
        )
        for d, k_ in out_pieces(p):
            start(hop(d, 1, k_))
        start(cross(0, 0, p, c))

    def blocks_of(h):
        if h == 0:
            return [(z * 2 + i, i) for i in (0, 1)]
        lo_ = from_chip(0, h)
        hi_ = from_chip(1, h)
        if h == far:
            return [(lo_ * 2 + i, 4 * h - 2 + i) for i in (0, 1)]
        return [(lo_ * 2 + i, 4 * h - 2 + i) for i in (0, 1)] + [
            (hi_ * 2 + i, 4 * h + i) for i in (0, 1)
        ]

    def hswap(b, i):
        return remote(hid.at[0, b], hid.at[1, b], hs_.at[i], hr_.at[i], sib)

    def run(h):
        for d in (0, 1):
            if h == 0 and d == 1:
                continue
            for p in pieces(d, h):
                cross(d, h, p, 1 - c).wait_recv()
        bl = blocks_of(h)
        xin = jnp.concatenate([rows[b] for b, i in bl], axis=0)
        g = dot(xin, gw[...])
        u = dot(xin, uw[...])
        hv = (g * jax.nn.sigmoid(g) * u).astype(BF)
        for j, (b, i) in enumerate(bl):
            hid[0, b] = hv[j * per : (j + 1) * per]
            start(hswap(b, i))

    def finish(h):
        bl = blocks_of(h)
        for b, i in bl:
            hswap(b, i).wait_recv()
        h0 = jnp.concatenate([hid[0, b] for b, i in bl], axis=0)
        h1 = jnp.concatenate([hid[1, b] for b, i in bl], axis=0)
        val = dot(h0, dw[...]) + dot(h1, dsib[...])
        for j, (b, i) in enumerate(bl):
            partc[b] = val[j * per : (j + 1) * per]

    loads[1].wait()
    loads[2].wait()
    for h in range(1, far + 1):
        for i in range(ROW_PIECES):
            for d in (0, 1):
                p = order(d)[i]
                if p not in pieces(d, h):
                    continue
                got_hop(d, h, p).wait_recv()
                if h + 1 <= far and p in pieces(d, h + 1):
                    start(hop(d, h + 1, p))
                start(cross(d, h, p, c))
            if i == 0:
                run(h - 1)
                if h == 1:
                    loads[3].wait()
                    remote(down.at[:, other_half], dsib, ws.at[1], wr.at[1], sib).wait_recv()
            if i == 1:
                finish(h - 1)
    chunk_c = 2 * per
    hc = chunk_c // BACK_PIECES

    def own_c(zz, p):
        b = zz * 2 + (p * hc) // per
        return partc[b, (p * hc) % per : (p * hc) % per + hc, :]

    def last_c(p, tot):
        core = (p * hc) // per
        e0 = ((p * hc) % per) // 2
        tb = tot.astype(BF)
        for e in range(hc // 2):
            t = e0 + e
            fin[core, t] = tb[2 * e : 2 * e + 2, :]
            ty, tx = t // nx, t % nx

            @pl.when(me != t)
            def _(t=t, ty=ty, tx=tx):
                remote(
                    fin.at[core, t], ret.at[c, me], fs.at[core, t], fr.at[c, me], (ty, tx, z, core)
                ).start()

            @pl.when((me == t) & (c != core))
            def _(t=t):
                remote(
                    fin.at[core, t], ret.at[c, me], fs.at[core, t], fr.at[c, me], sib
                ).start()

    back_ring = (own_c, sbc, rbc, ss, rs, BACK_PIECES, hc, last_c)
    ring_sum(*back_ring, begun=False)
    run(far)
    finish(far)
    ring_sum(*back_ring, begun=True)
    ret[c, me] = fin[c, me]
    for i in (0, 1):
        for t in range(n):

            @pl.when((me != t) | (c != i))
            def _(t=t, i=i):
                remote(fin.at[0, t], ret.at[i, t], fs.at[0, t], fr.at[i, t], sib).wait_recv()

            back[2 * t : 2 * t + 2, i * half : (i + 1) * half] = ret[i, t]
    for i in range(2):
        cols = slice(i * half, (i + 1) * half)
        bk = back[:, cols]
        mix = route[0] * dot(take[0], bk) + route[1] * dot(take[1], bk)
        out[:, cols] = mixed[:, cols].astype(F32) + mix

    for cond, copies in plan:

        @pl.when(cond)
        def _(copies=copies):
            for a in copies:
                a.wait_send()

    for core in (0, 1):
        for t in range(n):

            @pl.when((me != t) | (c != core))
            def _(t=t, core=core):
                remote(
                    fin.at[core, t], ret.at[c, me], fs.at[core, t], fr.at[c, me], sib
                ).wait_send()

    for a in sends:
        a.wait_send()


def per_device(
    residual_in, queries, keys, values, break_offset, doc_ids, out_weight, norm_gain,
    group_router, expert_router, expert_ids, gate_weight, up_weight, down_weight,
):
    ny, nx, nz = lax.axis_size("y"), lax.axis_size("x"), lax.axis_size("z")
    n = ny * nx
    rows, att = queries.shape
    tok, width = residual_in.shape
    half = width // 2
    heads = break_offset.shape[1]
    gate, up, down = gate_weight[0], up_weight[0], down_weight[0]
    units = gate.shape[1]
    per = 2 * n
    far = nz // 2
    sends = (nx - 1) + (ny - 1) + (nx - 1) * (ny - 1)
    dma = pltpu.SemaphoreType.DMA
    vm = pltpu.VMEM
    scratch = [
        vm((tok, width), BF), vm((rows, att), BF), vm((rows, att), BF), vm((rows, att), BF),
        vm((heads, rows), BF), vm((1, rows), jnp.int32), vm((1, width), F32),
        vm((2, rows), jnp.int32),
        vm((n, rows, att), BF), vm((n, rows, att), BF), vm((n, 16, rows), BF), vm((16, rows), BF),
        vm((KB, KB), BF), vm((rows, att), BF), vm((rows, 1), F32), vm((n, rows, att), F32),
        vm((n, heads, rows, 1), F32), vm((heads, rows, 1), F32), vm((rows, att), F32),
        vm((att, half), BF), vm((att, half), BF), vm((rows, att), BF), vm((rows, att), BF),
        vm((rows, half), F32),
        vm((2, far, rows // nz, half), BF), vm((2, far, rows // nz, half), BF),
        vm((tok, half), F32), vm((2, tok, half), F32), vm((tok, width), BF),
        vm((n, 2, width), BF), vm((n, 2, width), BF), vm((2 * nz, per, width), BF),
        vm((width, units), BF), vm((width, units), BF), vm((units, half), BF),
        vm((units, half), BF),
        vm((2, 2 * nz, per, units), BF), vm((2 * nz, per, half), F32),
        vm((2, far, 2 * per, half), BF), vm((2, far, 2 * per, half), BF),
        vm((2, n, 2, half), BF), vm((2, n, 2, half), BF), vm((per, width), BF),
        vm((GROUPS, width), BF), vm((n, width), BF),
        dma((14,)),
        dma((sends,)), dma((n,)), dma((sends,)), dma((n,)), dma((sends,)), dma((n,)),
        dma((2,)), dma((2,)), dma, dma,
        dma((2, far, SUM_PIECES)), dma((2, far, SUM_PIECES)), dma, dma,
        dma((n - 1,)), dma((n,)),
        dma((2, far + 1, ROW_PIECES)), dma((2, far + 1, ROW_PIECES)),
        dma((2, far + 1, ROW_PIECES)), dma((2, far + 1, ROW_PIECES)),
        dma((2 * nz,)), dma((2 * nz,)),
        dma((2, far, BACK_PIECES)), dma((2, far, BACK_PIECES)),
        dma((2, n)), dma((2, n)),
    ]
    summed = pl.pallas_call(
        functools.partial(layer_kernel, (ny, nx, nz)),
        out_shape=jax.ShapeDtypeStruct(residual_in.shape, F32),
        in_specs=[ANY] * 14,
        out_specs=VM,
        scratch_shapes=scratch,
        compiler_params=pltpu.CompilerParams(
            collective_id=1, has_side_effects=True, vmem_limit_bytes=LIMIT
        ),
        name="layer",
    )(
        residual_in, queries, keys, values, break_offset.T, doc_ids[None, :], out_weight,
        norm_gain[None, :], group_router.T, expert_router.T, expert_ids.T, gate, up, down,
    )
    return summed.astype(BF)


def solution(mesh):
    n = mesh.shape["sp"]
    side = round(n**0.5)
    finer = Mesh(mesh.devices.reshape(side, n // side, mesh.shape["tp"] // 2, 2), AXES)
    in_specs = (
        P(SP + TP, None),
        P(SP, TP),
        P(SP, TP),
        P(SP, TP),
        P(SP, TP),
        P(SP),
        P(TP, None),
        P(),
        P(),
        P(),
        P(SP, None),
        P(SP, None, TP),
        P(SP, None, TP),
        P(SP, TP, None),
    )
    return jax.shard_map(
        per_device, mesh=finer, in_specs=in_specs, out_specs=P(SP + TP, None), check_vma=False
    )
```
